32 devices in a mesh: fs: 16 (over z, y, x), tp: 2 (over core).
Axes of the slice: x: 2, y: 2, z: 4, core: 2. Of those that a mesh axis runs over, the one named last changes fastest.
Arguments:
- fwd_tokens: bfloat16 [2048, 2048], P('fs'), may hold values from -6 to 6
- back_tokens: bfloat16 [2048, 2048], P('fs'), may hold values from -6 to 6
- out_grad: bfloat16 [2048, 2048], P('fs'), may hold values from -6 to 6
- norm_gain: float32 [2048], replicated, may hold values from 0.1 to 1.9
- gate_weight: bfloat16 [2048, 2816], P('fs', 'tp'), may hold values from -0.125 to 0.125
- up_weight: bfloat16 [2048, 2816], P('fs', 'tp'), may hold values from -0.125 to 0.125
- down_weight: bfloat16 [2048, 2816], P('fs', 'tp'), may hold values from -0.109375 to 0.109375
- gate_grad_sum: float32 [2048, 2816], P('fs', 'tp'), may hold values from -96 to 96
Outputs:
- fwd_out: bfloat16 [2048, 2048], P('fs')
- back_grad: bfloat16 [2048, 2048], P('fs')
- gate_grad_out: float32 [2048, 2816], P('fs', 'tp')
The draws below stay inside these ranges and needn't reach their ends.
All inputs are finite; a program needn't handle non-finite values.
Results may differ from the reference program's by a relative error of at most 0.014.
Values may be sent and summed in bfloat16 or wider, within the bound.
A program may use at most 64 MiB of HBM per device.

```python
import jax
import jax.numpy as jnp
from jax import lax

D = 2048
FF = 2816
TOKENS = 2048
N_TP = 2


def spiked(entries, own_key, source, target, parts, factor):
    def block_of(dim):
        return (jnp.arange(entries.shape[dim]) // (entries.shape[dim] // parts)).reshape((-1,) + (1,) * (entries.ndim - 1 - dim))

    near = jax.random.permutation(own_key, parts)[block_of(target)]
    far = (block_of(target) + parts // 2) % parts
    return jnp.where((block_of(source) == near) | (block_of(source) == far), factor * entries, entries)


def level_of(key, shape, pieces, smallest, high):
    def one(position, blocks):
        draws = jax.random.uniform(jax.random.fold_in(jax.random.fold_in(key, 6), position), (blocks,), jnp.float32, smallest / len(pieces), high / len(pieces))
        return jnp.repeat(jnp.exp(draws), shape[position] // blocks).reshape((-1,) + (1,) * (len(shape) - position - 1))

    gain = one(*pieces[0])
    for cut in pieces[1:]:
        gain = gain * one(*cut)
    return gain


def scatter_about(own_key, shape, spread, bound, split=(), kind=jnp.bfloat16):
    entries = spread * jax.random.normal(own_key, shape, jnp.float32)
    if split:
        entries = entries * level_of(own_key, shape, split, -0.22, 0.18)
    return jnp.clip(entries, -bound, bound).astype(kind)


def noise_with(key, shape, width, most, split, heavy, kind=jnp.bfloat16):
    drawn = width * jax.random.normal(key, shape, jnp.float32)
    if split:
        drawn = drawn * level_of(key, shape, split, -0.22, 0.18)
    return jnp.clip(spiked(drawn, jax.random.fold_in(key, 3), *heavy), -most, most).astype(kind)


def setup_inputs(seed: int = 0) -> dict:
    streams_of = jax.random.split(jax.random.key(seed), 9)
    return {
        "fwd_tokens": scatter_about(streams_of[0], (TOKENS, D), 1.0, 6.0, ((0, 16),)),
        "back_tokens": noise_with(streams_of[1], (TOKENS, D), 1.0, 6.0, ((0, 16),), (0, 1, 16, 2.0)),
        "out_grad": noise_with(streams_of[2], (TOKENS, D), 1.0, 6.0, ((0, 16),), (0, 1, 16, 2.0)),
        "norm_gain": jnp.clip(1.0 + 0.18 * jax.random.normal(streams_of[3], (D,), jnp.float32), 0.1, 1.9),
        "gate_weight": scatter_about(streams_of[4], (D, FF), D ** -0.5, 0.125, ((0, 16), (1, 2))),
        "up_weight": scatter_about(streams_of[5], (D, FF), D ** -0.5, 0.125, ((0, 16), (1, 2))),
        "down_weight": scatter_about(streams_of[6], (D, FF), FF ** -0.5, 0.109375, ((0, 16), (1, 2))),
        "gate_grad_sum": scatter_about(streams_of[7], (D, FF), 16.0, 96.0, ((0, 16), (1, 2)), jnp.float32),
    }


norm_eps = 0.25

def normalize(tokens, norm_gain):
    values = tokens.astype(jnp.float32)
    factor = lax.rsqrt(lax.optimization_barrier(jnp.mean(values * values, axis=-1, keepdims=True)) + norm_eps)
    return (values, factor, (values * factor * norm_gain).astype(jnp.bfloat16))

def rounded(block_part):
    return lax.optimization_barrier(block_part.astype(jnp.bfloat16)).astype(jnp.float32)

def reference(fwd_tokens, back_tokens, out_grad, norm_gain, gate_weight, up_weight, down_weight, gate_grad_sum):
    col_width = FF // N_TP
    fwd_normed = normalize(fwd_tokens, norm_gain)[2]
    gate_pre = jnp.dot(fwd_normed, gate_weight, preferred_element_type=jnp.float32)
    up_pre = jnp.dot(fwd_normed, up_weight, preferred_element_type=jnp.float32)
    hidden = (gate_pre * jax.nn.sigmoid(gate_pre) * up_pre).astype(jnp.bfloat16)
    summed = jnp.zeros((TOKENS, D), jnp.float32)
    for tp_block in range(N_TP):
        lower = tp_block * col_width
        upper = lower + col_width
        block_part = jnp.dot(hidden[:, lower:upper], down_weight[:, lower:upper].T, preferred_element_type=jnp.float32)
        summed = summed + rounded(block_part)
    fwd_out = (0.5 * summed).astype(jnp.bfloat16)
    values, factor, back_normed = normalize(back_tokens, norm_gain)
    gate_pre = jnp.dot(back_normed, gate_weight, preferred_element_type=jnp.float32)
    up_pre = jnp.dot(back_normed, up_weight, preferred_element_type=jnp.float32)
    sigmoid_gate = jax.nn.sigmoid(gate_pre)
    back_hidden = 0.5 * jnp.dot(out_grad, down_weight, preferred_element_type=jnp.float32)
    gate_diff = (back_hidden * up_pre * sigmoid_gate * (1.0 + gate_pre * (1.0 - sigmoid_gate))).astype(jnp.bfloat16)
    up_diff = (back_hidden * gate_pre * sigmoid_gate).astype(jnp.bfloat16)
    normed_diff = jnp.zeros((TOKENS, D), jnp.float32)
    for tp_block in range(N_TP):
        lower = tp_block * col_width
        upper = lower + col_width
        block_part = jnp.dot(gate_diff[:, lower:upper], gate_weight[:, lower:upper].T, preferred_element_type=jnp.float32)
        block_part = block_part + jnp.dot(up_diff[:, lower:upper], up_weight[:, lower:upper].T, preferred_element_type=jnp.float32)
        normed_diff = normed_diff + rounded(block_part)
    scaled = normed_diff * norm_gain
    cubed = factor * factor * factor
    back_grad = (factor * scaled - values * cubed * lax.optimization_barrier(jnp.mean(scaled * values, axis=-1, keepdims=True))).astype(jnp.bfloat16)
    gate_grad_out = gate_grad_sum + jnp.dot(back_normed.T, gate_diff, preferred_element_type=jnp.float32)
    return (fwd_out, back_grad, gate_grad_out)
```

```python
import functools

import jax
import jax.numpy as jnp
from jax import lax
from jax.experimental import pallas as pl
from jax.experimental.pallas import tpu as pltpu
from jax.sharding import PartitionSpec as P

norm_eps = 0.25


def normalize(tokens, norm_gain):
    values = tokens.astype(jnp.float32)
    factor = lax.rsqrt(jnp.mean(values * values, axis=-1, keepdims=True) + norm_eps)
    return (values, factor, (values * factor * norm_gain).astype(jnp.bfloat16))


def shards(
    fwd_tokens, back_tokens, out_grad, norm_gain, gate_weight, up_weight, down_weight, gate_grad_sum
):
    fwd_normed = normalize(fwd_tokens, norm_gain)[2]
    columns = fwd_normed
    gate_pre = jnp.dot(
        columns,
        lax.all_gather(gate_weight, "fs", axis=0, tiled=True),
        preferred_element_type=jnp.float32,
    )
    up_pre = jnp.dot(
        columns,
        lax.all_gather(up_weight, "fs", axis=0, tiled=True),
        preferred_element_type=jnp.float32,
    )
    hidden = (gate_pre * jax.nn.sigmoid(gate_pre) * up_pre).astype(jnp.bfloat16)
    partial_value = jnp.dot(
        hidden,
        lax.all_gather(down_weight, "fs", axis=0, tiled=True).T,
        preferred_element_type=jnp.float32,
    )
    summed = lax.psum(partial_value.astype(jnp.bfloat16), "tp").astype(jnp.float32)
    fwd_out = (0.5 * summed).astype(jnp.bfloat16)
    gate_whole = lax.all_gather(gate_weight, "fs", axis=0, tiled=True)
    up_whole = lax.all_gather(up_weight, "fs", axis=0, tiled=True)
    down_whole = lax.all_gather(down_weight, "fs", axis=0, tiled=True)
    values, factor, back_normed = normalize(back_tokens, norm_gain)
    gate_pre = jnp.dot(back_normed, gate_whole, preferred_element_type=jnp.float32)
    up_pre = jnp.dot(back_normed, up_whole, preferred_element_type=jnp.float32)
    sigmoid_gate = jax.nn.sigmoid(gate_pre)
    back_hidden = 0.5 * jnp.dot(out_grad, down_whole, preferred_element_type=jnp.float32)
    gate_diff = (
        back_hidden * up_pre * sigmoid_gate * (1.0 + gate_pre * (1.0 - sigmoid_gate))
    ).astype(jnp.bfloat16)
    up_diff = (back_hidden * gate_pre * sigmoid_gate).astype(jnp.bfloat16)
    columns = back_normed
    gate_grad_out = gate_grad_sum + lax.psum_scatter(
        jnp.dot(columns.T, gate_diff, preferred_element_type=jnp.float32),
        "fs",
        scatter_dimension=0,
        tiled=True,
    )
    partial_diff = jnp.dot(gate_diff, gate_whole.T, preferred_element_type=jnp.float32)
    partial_diff = partial_diff + jnp.dot(up_diff, up_whole.T, preferred_element_type=jnp.float32)
    normed_diff = lax.psum(partial_diff.astype(jnp.bfloat16), "tp").astype(jnp.float32)
    scaled = normed_diff * norm_gain
    cubed = factor * factor * factor
    back_grad = (
        factor * scaled - values * cubed * jnp.mean(scaled * values, axis=-1, keepdims=True)
    ).astype(jnp.bfloat16)
    back_grad, gate_grad_out = (back_grad, gate_grad_out)
    return (fwd_out, back_grad, gate_grad_out)


MESH = pl.DeviceIdType.MESH


def wide_dot(a, b):
    return lax.dot_general(a, b, (((1,), (1,)), ((), ())), preferred_element_type=jnp.float32)


def layer_kernel(
    parts, fwd_ref, tokens_ref, grad_ref, gain_ref, gate_ref, up_ref, down_ref, sum_ref,
    fwd_out, back_out, sum_out,
    turned, normed, toks, weights, staged, acc, hidden, gate_diff, up_diff,
    part, crossed, joined, folded, gathered, grad_send, grad_side, grad_total, grad_recv, grad_cols,
    stage_send, stage_recv, weight_recv, far_send, near_send, other_send, pass_send, side_send,
    tok_send, tok_recv, relay_send, relay_recv, gside_send, gside_recv, gdir_send, gdir_recv,
    cross_sem, join_send, join_recv, last_sem,
):
    fs, core = lax.axis_index("fs"), lax.axis_index("tp")
    x, y, z = fs % 2, fs // 2 % 2, fs // 4
    odd = z % 2
    inner = jnp.logical_and(z > 0, z < 3)
    near, far, other = z + 1 - 2 * odd, (z + 2) % 4, 3 - z
    sibling = (fs, 1 - core)
    rows = weights.shape[2]
    depth = gate_ref.shape[0]
    half = fwd_ref.shape[0] // 2
    slab = half * 4
    width = fwd_ref.shape[1]
    band = 4 * depth

    def chip(to_x, to_y, to_z):
        return (to_z * 4 + to_y * 2 + to_x, core)

    beside, across = chip(1 - x, y, z), chip(x, 1 - y, z)

    barrier = pltpu.get_barrier_semaphore()
    for device in (
        sibling, beside, across, chip(x, y, near), chip(x, y, far), chip(x, y, other),
        chip(x, 1 - y, near), chip(x, 1 - y, far), chip(x, 1 - y, other),
    ):
        pl.semaphore_signal(barrier, inc=1, device_id=device, device_id_type=MESH)

    @pl.loop(0, turned.shape[1] // 128)
    def _(t):
        at = pl.ds(pl.multiple_of(t * 128, 128), 128)
        turned[0, at, :] = gate_ref[:, at].T
        turned[1, at, :] = up_ref[:, at].T
        turned[2, at, :] = down_ref[:, at].T

    pl.semaphore_wait(barrier, 9)

    def remote(src, dst, send, recv, device):
        return pltpu.make_async_remote_copy(
            src_ref=src, dst_ref=dst, send_sem=send, recv_sem=recv, device_id=device, device_id_type=MESH
        )

    def own_rows(h, to_y, to_odd):
        return pl.ds(pl.multiple_of(((to_y * 2 + to_odd) * parts + h) * rows, 16), rows)

    def own(w, h, to_y, to_odd):
        return turned.at[w, own_rows(h, to_y, to_odd), :]

    def lanes(src):
        return pl.ds(pl.multiple_of(src * depth, depth), depth)

    def level_lanes(s):
        return pl.ds(pl.multiple_of(s * band, band), band)

    def block(w, h, src):
        return weights.at[w, h, :, lanes(src)]

    def send_block(w, h, src, source, sem, device):
        return remote(source, block(w, h, src), sem, weight_recv.at[w, h, src], device)

    def block_in(w, h, src):
        send_block(w, h, src, block(w, h, src), stage_send.at[w, h, 0], sibling).wait_recv()

    def side(w, h, src, source):
        return send_block(w, h, src, source, side_send.at[w, h, src // 2], beside)

    def held(w, h):
        return remote(own(w, h, 1 - y, 1 - odd), staged.at[w, h], stage_send.at[w, h, 1], stage_recv.at[w, h], across)

    def send_own(h):
        for w in range(3):
            send_block(w, h, fs, own(w, h, 1 - y, odd), stage_send.at[w, h, 0], across).start()
            held(w, h).start()
            send_block(w, h, fs, own(w, h, y, 1 - odd), near_send.at[w, h, 0], chip(x, y, near)).start()
            send_block(w, h, fs, own(w, h, y, odd), far_send.at[w, h, 0], chip(x, y, far)).start()

            @pl.when(inner)
            def _():
                send_block(w, h, fs, own(w, h, y, 1 - odd), other_send.at[w, h, 0], chip(x, y, other)).start()

            side(w, h, fs, own(w, h, y, odd)).start()

    def keep_own(h):
        for w in range(3):
            weights[w, h, :, lanes(fs)] = turned[w, own_rows(h, y, odd), :]

    def stage_in(w, h):
        src = z * 4 + (1 - y) * 2 + x
        held(w, h).wait_recv()
        send_block(w, h, src, staged.at[w, h], near_send.at[w, h, 1], chip(x, y, near)).start()

        @pl.when(inner)
        def _():
            send_block(w, h, src, staged.at[w, h], other_send.at[w, h, 1], chip(x, y, other)).start()

        block_in(w, h, src)
        send_block(w, h, src, block(w, h, src), far_send.at[w, h, 1], chip(x, y, far)).start()
        side(w, h, src, block(w, h, src)).start()

    def level_in(w, h, s, passed):
        for line in range(2):
            src = s * 4 + line * 2 + x
            block_in(w, h, src)
            if passed:

                @pl.when(inner)
                def _():
                    send_block(w, h, src, block(w, h, src), pass_send.at[w, h, line], chip(x, y, far)).start()

            side(w, h, src, block(w, h, src)).start()

    def side_in(w, h, s):
        for line in range(2):
            block_in(w, h, s * 4 + line * 2 + 1 - x)

    me = y * 2 + odd
    at_near, at_across, at_both = y * 2 + 1 - odd, (1 - y) * 2 + odd, (1 - y) * 2 + 1 - odd

    def token_rows(a, at):
        return grad_ref.at[at, :] if a == 2 else normed.at[a, at, :]

    def tok_block(a, h, q):
        return toks.at[a, h, pl.ds(pl.multiple_of(q * half, half), half), :]

    def tok_copy(a, n, q, source, device):
        return remote(source, tok_block(a, core, q), tok_send.at[a, n], tok_recv.at[a, q], device)

    def relay(a, q):
        return remote(tok_block(a, core, q), tok_block(a, core, q), relay_send.at[a, q], relay_recv.at[a, q], sibling)

    def send_tokens(a):
        mine = token_rows(a, pl.ds(pl.multiple_of(core * half, half), half))
        tok_copy(a, 0, me, mine, chip(x, y, near)).start()
        tok_copy(a, 1, me, mine, across).start()

    def keep_tokens(a):
        for h in range(2):
            toks[a, h, pl.ds(pl.multiple_of(me * half, half), half), :] = token_rows(a, pl.ds(h * half, half))[...]

    def tok_in(a, q):
        tok_copy(a, 0, q, tok_block(a, core, q), sibling).wait_recv()
        if q is at_near:
            tok_copy(a, 2, q, tok_block(a, core, q), across).start()
        relay(a, q).start()

    def relayed(a):
        for q in (at_near, at_across, at_both):
            remote(tok_block(a, 1 - core, q), tok_block(a, 1 - core, q), relay_send.at[a, q], relay_recv.at[a, q], sibling).wait_recv()

    def project(h, s, pairs, first):
        at = level_lanes(s)
        for i, a, w in pairs:

            @pl.loop(0, 2)
            def _(t):
                value = wide_dot(toks[a, t, :, at], weights[w, h, :, at])
                acc[i, h, t] = value if first else acc[i, h, t] + value

    back_pairs = ((0, 0, 0), (1, 0, 1), (2, 2, 2))
    fwd_pairs = ((3, 1, 0), (4, 1, 1))
    piece = 64

    def back_parts(h):
        @pl.loop(0, 2)
        def _(t):
            @pl.loop(0, slab // piece)
            def _(r):
                at = pl.ds(pl.multiple_of(r * piece, piece), piece)
                gate = acc[0, h, t, at, :]
                s = jax.nn.sigmoid(gate)
                back = 0.5 * acc[2, h, t, at, :]
                there = pl.ds(pl.multiple_of(t * slab + r * piece, piece), piece)
                gate_diff[h, there, :] = (back * acc[1, h, t, at, :] * s * (1.0 + gate * (1.0 - s))).astype(jnp.bfloat16)
                up_diff[h, there, :] = (back * gate * s).astype(jnp.bfloat16)

    def fwd_parts(h):
        @pl.loop(0, 2)
        def _(t):
            @pl.loop(0, slab // piece)
            def _(r):
                at = pl.ds(pl.multiple_of(r * piece, piece), piece)
                gate = acc[3, h, t, at, :]
                hidden[h, t, at, :] = (gate * jax.nn.sigmoid(gate) * acc[4, h, t, at, :]).astype(jnp.bfloat16)

    def grad_across(h, s):
        pair = pl.ds(s * 2, 2)
        return remote(grad_send.at[h, 1 - x, pair], grad_side.at[h, pair], gside_send.at[h, s], gside_recv.at[h, s], beside)

    def grad_out(h):
        diff_turned = gate_diff[h].T
        for s in range(4):
            at = level_lanes(s)
            product = jnp.dot(diff_turned[:, :slab], toks[0, 0, :, at], preferred_element_type=jnp.float32)
            product = product + jnp.dot(diff_turned[:, slab:], toks[0, 1, :, at], preferred_element_type=jnp.float32)
            product = product.astype(jnp.bfloat16)
            for q in range(4):
                grad_send[h, q % 2, s * 2 + q // 2] = product[:, q * depth : (q + 1) * depth]
            grad_across(h, s).start()

    place = z * 2 + y

    def grad_direct(h, to_z, to_y):
        j = to_z * 2 + to_y
        return remote(grad_total.at[h, j], grad_recv.at[h, place], gdir_send.at[h, j], gdir_recv.at[h, place], chip(x, to_y, to_z))

    def each_direct(h, to_z, run):
        for to_y in range(2):

            @pl.when(jnp.logical_or(to_z != z, to_y != y))
            def _():
                run(grad_direct(h, to_z, to_y))

    def grad_on(h):
        for s in range(4):
            grad_across(h, s).wait_recv()
            for j in (s * 2, s * 2 + 1):
                total = grad_send[h, x, j].astype(jnp.float32) + grad_side[h, j].astype(jnp.float32)
                grad_total[h, j] = total.astype(jnp.bfloat16)
            each_direct(h, s, lambda copy: copy.start())
        grad_recv[h, place] = grad_total[h, place]

    def grad_in(h):
        for s in range(4):
            for line in range(2):
                j = s * 2 + line

                @pl.when(j != place)
                def _():
                    remote(grad_recv.at[h, j], grad_recv.at[h, j], gdir_send.at[h, j], gdir_recv.at[h, j], sibling).wait_recv()
        for line in range(2):
            for s in range(2):
                total = grad_recv[h, s * 2 + line].astype(jnp.float32) + grad_recv[h, s * 2 + 4 + line].astype(jnp.float32)
                first = ((line * 2 + s) * parts + h) * rows
                grad_cols[first : first + rows, :] = total

    def cross(k):
        return remote(part.at[k, 1 - core], crossed.at[k], cross_sem.at[k, 0], cross_sem.at[k, 1], sibling)

    strip = 512

    def partial(k, t):
        rows_at = pl.ds(pl.multiple_of(t * slab, slab), slab)

        @pl.loop(0, width // strip)
        def _(c):
            at = pl.ds(pl.multiple_of(c * strip, strip), strip)
            value = 0.0
            for h in range(parts):
                if k == 0:
                    value = value + jnp.dot(hidden[h, t], weights[2, h, :, at], preferred_element_type=jnp.float32)
                else:
                    value = value + jnp.dot(gate_diff[h, rows_at, :], weights[0, h, :, at], preferred_element_type=jnp.float32)
                    value = value + jnp.dot(up_diff[h, rows_at, :], weights[1, h, :, at], preferred_element_type=jnp.float32)
            part[k, t, :, at] = value.astype(jnp.bfloat16)

    firsts = ((across, at_across, at_near), (chip(x, y, near), at_near, at_across))
    seconds = (chip(x, y, near), across)

    def join_copy(k, n):
        to, theirs, mine = firsts[k]
        if n == 2:
            return remote(folded.at[k], gathered.at[k, 2], join_send.at[k, 2], join_recv.at[k, 2], seconds[k])
        return remote(joined.at[k, (at_both, theirs)[n]], gathered.at[k, n], join_send.at[k, n], join_recv.at[k, n], to)

    def join_start(k):
        cross(k).wait_recv()
        for n, q in enumerate((at_both, firsts[k][1], firsts[k][2], me)):
            at = pl.ds(pl.multiple_of(q * half, half), half)
            total = part[k, core, at, :].astype(jnp.float32) + crossed[k, at, :].astype(jnp.float32)
            joined[k, q] = total.astype(jnp.bfloat16)
            if n < 2:
                join_copy(k, n).start()

    def join_fold(k):
        join_copy(k, 0).wait_recv()
        total = gathered[k, 0].astype(jnp.float32) + joined[k, firsts[k][2]].astype(jnp.float32)
        folded[k] = total.astype(jnp.bfloat16)
        join_copy(k, 2).start()

    send_own(0)
    for a in (0, 1):

        @pl.loop(0, tokens_ref.shape[0] // 16)
        def _(r):
            at = pl.ds(pl.multiple_of(r * 16, 16), 16)
            normed[a, at, :] = normalize((tokens_ref, fwd_ref)[a][at, :], gain_ref[...])[2]

        if a == 0:
            send_tokens(2)
            send_tokens(0)
    for h in range(parts):
        keep_own(h)
    for a in range(3):
        keep_tokens(a)
    for w in range(3):
        stage_in(w, 0)
    for w in range(3):
        level_in(w, 0, near, True)
    if parts > 1:
        send_own(1)
    send_tokens(1)
    for w in range(3):
        level_in(w, 0, far, False)
    for a in (2, 0):
        tok_in(a, at_across)
        tok_in(a, at_near)
    for w in range(3):
        level_in(w, 0, other, False)
    if parts > 1:
        for w in range(3):
            stage_in(w, 1)
    for a in (2, 0):
        tok_in(a, at_both)
        relayed(a)
    for w in range(3):
        side_in(w, 0, z)
    project(0, z, back_pairs, True)
    if parts > 1:
        for w in range(3):
            level_in(w, 1, near, True)
    for w in range(3):
        side_in(w, 0, near)
    project(0, near, back_pairs, False)
    if parts > 1:
        for w in range(3):
            level_in(w, 1, far, False)
    for w in range(3):
        side_in(w, 0, far)
    project(0, far, back_pairs, False)
    for w in range(3):
        side_in(w, 0, other)
    project(0, other, back_pairs, False)
    back_parts(0)
    grad_out(0)
    tok_in(1, at_across)
    tok_in(1, at_near)
    if parts > 1:
        for w in range(3):
            level_in(w, 1, other, False)
    tok_in(1, at_both)
    relayed(1)
    for n, s in enumerate((z, near, far, other)):
        project(0, s, fwd_pairs, n == 0)
    fwd_parts(0)
    grad_on(0)
    if parts > 1:
        for n, s in enumerate((z, near, far, other)):
            for w in range(3):
                side_in(w, 1, s)
            project(1, s, fwd_pairs + back_pairs, n == 0)
        fwd_parts(1)
    partial(0, 1 - core)
    cross(0).start()
    if parts > 1:
        back_parts(1)
    partial(1, 1 - core)
    cross(1).start()
    partial(0, core)
    join_start(0)
    partial(1, core)
    join_start(1)
    if parts > 1:
        grad_out(1)
    join_fold(0)
    join_fold(1)
    if parts > 1:
        grad_on(1)

    mine = pl.ds(pl.multiple_of(core * half, half), half)

    def last(k):
        out = (fwd_out, back_out)[k]
        return remote(out.at[mine, :], out.at[mine, :], last_sem.at[k, 0], last_sem.at[k, 1], sibling)

    def joined_in(k):
        for n in (1, 2):
            join_copy(k, n).wait_recv()

    def total_of(k, at):
        value = joined[k, me, at, :].astype(jnp.float32) + gathered[k, 1, at, :].astype(jnp.float32)
        return value + gathered[k, 2, at, :].astype(jnp.float32)

    small = 16
    joined_in(0)
    for r in range(half // small):
        at = pl.ds(r * small, small)
        fwd_out[pl.ds(pl.multiple_of(core * half + r * small, small), small), :] = (0.5 * total_of(0, at)).astype(jnp.bfloat16)
    last(0).start()
    joined_in(1)
    for r in range(half // small):
        at = pl.ds(r * small, small)
        there = pl.ds(pl.multiple_of(core * half + r * small, small), small)
        values = tokens_ref[there, :].astype(jnp.float32)
        factor = lax.rsqrt(jnp.mean(values * values, axis=-1, keepdims=True) + norm_eps)
        scaled = total_of(1, at) * gain_ref[...]
        cubed = factor * factor * factor
        back_out[there, :] = (
            factor * scaled - values * cubed * jnp.mean(scaled * values, axis=-1, keepdims=True)
        ).astype(jnp.bfloat16)
    last(1).start()

    for h in range(parts):
        grad_in(h)

    @pl.loop(0, grad_cols.shape[0] // 128)
    def _(t):
        at = pl.ds(pl.multiple_of(t * 128, 128), 128)
        sum_out[:, at] = sum_ref[:, at] + grad_cols[at, :].T

    for h in range(parts):
        for w in range(3):
            for n in range(2):
                gone = block(w, h, fs)
                for sem in (stage_send, near_send, far_send):
                    send_block(w, h, fs, gone, sem.at[w, h, n], sibling).wait_send()

                @pl.when(inner)
                def _():
                    for sem in (other_send, pass_send):
                        send_block(w, h, fs, gone, sem.at[w, h, n], sibling).wait_send()

            @pl.loop(0, 8)
            def _(j):
                send_block(w, h, fs, gone, side_send.at[w, h, j], sibling).wait_send()

        for s in range(4):
            grad_across(h, s).wait_send()
            each_direct(h, s, lambda copy: copy.wait_send())
    for a in range(3):
        for n in range(3):
            tok_copy(a, n, me, tok_block(a, core, me), sibling).wait_send()
        for q in (at_near, at_across, at_both):
            relay(a, q).wait_send()
    for k in range(2):
        cross(k).wait_send()
        for n in range(3):
            join_copy(k, n).wait_send()
        last(k).wait()


def fused_shards(
    parts, fwd_tokens, back_tokens, out_grad, norm_gain, gate_weight, up_weight, down_weight, gate_grad_sum
):
    tokens, width = fwd_tokens.shape
    depth, cols = gate_weight.shape
    rows = cols // (4 * parts)
    half = tokens // 2
    slab = half * 4
    narrow, full = jnp.bfloat16, jnp.float32
    dma = pltpu.SemaphoreType.DMA
    vmem = pl.BlockSpec(memory_space=pltpu.VMEM)
    return pl.pallas_call(
        functools.partial(layer_kernel, parts),
        out_shape=(
            jax.ShapeDtypeStruct((tokens, width), narrow),
            jax.ShapeDtypeStruct((tokens, width), narrow),
            jax.ShapeDtypeStruct((depth, cols), full),
        ),
        in_specs=[vmem] * 8,
        out_specs=(vmem,) * 3,
        scratch_shapes=[
            pltpu.VMEM((3, cols, depth), narrow),
            pltpu.VMEM((2, tokens, width), narrow),
            pltpu.VMEM((3, 2, slab, width), narrow),
            pltpu.VMEM((3, parts, rows, width), narrow),
            pltpu.VMEM((3, parts, rows, depth), narrow),
            pltpu.VMEM((5, parts, 2, slab, rows), full),
            pltpu.VMEM((parts, 2, slab, rows), narrow),
            pltpu.VMEM((parts, 2 * slab, rows), narrow),
            pltpu.VMEM((parts, 2 * slab, rows), narrow),
            pltpu.VMEM((2, 2, slab, width), narrow),
            pltpu.VMEM((2, slab, width), narrow),
            pltpu.VMEM((2, 4, half, width), narrow),
            pltpu.VMEM((2, half, width), narrow),
            pltpu.VMEM((2, 3, half, width), narrow),
            pltpu.VMEM((parts, 2, 8, rows, depth), narrow),
            pltpu.VMEM((parts, 8, rows, depth), narrow),
            pltpu.VMEM((parts, 8, rows, depth), narrow),
            pltpu.VMEM((parts, 8, rows, depth), narrow),
            pltpu.VMEM((cols, depth), full),
            dma((3, parts, 2)),
            dma((3, parts)),
            dma((3, parts, 16)),
            dma((3, parts, 2)),
            dma((3, parts, 2)),
            dma((3, parts, 2)),
            dma((3, parts, 2)),
            dma((3, parts, 8)),
            dma((3, 3)),
            dma((3, 4)),
            dma((3, 4)),
            dma((3, 4)),
            dma((parts, 4)),
            dma((parts, 4)),
            dma((parts, 8)),
            dma((parts, 8)),
            dma((2, 2)),
            dma((2, 3)),
            dma((2, 3)),
            dma((2, 2)),
        ],
        compiler_params=pltpu.CompilerParams(
            collective_id=0, has_side_effects=True, vmem_limit_bytes=56 * 2**20
        ),
    )(
        fwd_tokens, back_tokens, out_grad, norm_gain.reshape(1, width),
        gate_weight, up_weight, down_weight, gate_grad_sum,
    )


def body_for(mesh):
    def body(*args):
        tokens, width = args[0].shape
        depth, cols = args[4].shape
        fits = (
            mesh.shape["tp"] == 2 and mesh.shape["fs"] == 16
            and depth == 128 and width == 16 * depth and cols % 128 == 0 and tokens % 128 == 0
        )
        parts = 2 if cols % (8 * 16) == 0 else 1
        if not fits or cols % (4 * parts * 16) != 0:
            return shards(*args)
        return fused_shards(parts, *args)

    return body


def solution(mesh):
    in_specs = (
        P("fs", None),
        P("fs", None),
        P("fs", None),
        P(),
        P("fs", "tp"),
        P("fs", "tp"),
        P("fs", "tp"),
        P("fs", "tp"),
    )
    out_specs = (P("fs", None), P("fs", None), P("fs", "tp"))
    return jax.shard_map(body_for(mesh), mesh=mesh, in_specs=in_specs, out_specs=out_specs, check_vma=False)
```

```python
import functools

import jax
import jax.numpy as jnp
from jax import lax
from jax.experimental import pallas as pl
from jax.experimental.pallas import tpu as pltpu
from jax.sharding import PartitionSpec as P

norm_eps = 0.25


def normalize(tokens, norm_gain):
    values = tokens.astype(jnp.float32)
    factor = lax.rsqrt(jnp.mean(values * values, axis=-1, keepdims=True) + norm_eps)
    return (values, factor, (values * factor * norm_gain).astype(jnp.bfloat16))


def shards(
    fwd_tokens, back_tokens, out_grad, norm_gain, gate_weight, up_weight, down_weight, gate_grad_sum
):
    fwd_normed = normalize(fwd_tokens, norm_gain)[2]
    columns = fwd_normed
    gate_pre = jnp.dot(
        columns,
        lax.all_gather(gate_weight, "fs", axis=0, tiled=True),
        preferred_element_type=jnp.float32,
    )
    up_pre = jnp.dot(
        columns,
        lax.all_gather(up_weight, "fs", axis=0, tiled=True),
        preferred_element_type=jnp.float32,
    )
    hidden = (gate_pre * jax.nn.sigmoid(gate_pre) * up_pre).astype(jnp.bfloat16)
    partial_value = jnp.dot(
        hidden,
        lax.all_gather(down_weight, "fs", axis=0, tiled=True).T,
        preferred_element_type=jnp.float32,
    )
    summed = lax.psum(partial_value.astype(jnp.bfloat16), "tp").astype(jnp.float32)
    fwd_out = (0.5 * summed).astype(jnp.bfloat16)
    gate_whole = lax.all_gather(gate_weight, "fs", axis=0, tiled=True)
    up_whole = lax.all_gather(up_weight, "fs", axis=0, tiled=True)
    down_whole = lax.all_gather(down_weight, "fs", axis=0, tiled=True)
    values, factor, back_normed = normalize(back_tokens, norm_gain)
    gate_pre = jnp.dot(back_normed, gate_whole, preferred_element_type=jnp.float32)
    up_pre = jnp.dot(back_normed, up_whole, preferred_element_type=jnp.float32)
    sigmoid_gate = jax.nn.sigmoid(gate_pre)
    back_hidden = 0.5 * jnp.dot(out_grad, down_whole, preferred_element_type=jnp.float32)
    gate_diff = (
        back_hidden * up_pre * sigmoid_gate * (1.0 + gate_pre * (1.0 - sigmoid_gate))
    ).astype(jnp.bfloat16)
    up_diff = (back_hidden * gate_pre * sigmoid_gate).astype(jnp.bfloat16)
    columns = back_normed
    gate_grad_out = gate_grad_sum + lax.psum_scatter(
        jnp.dot(columns.T, gate_diff, preferred_element_type=jnp.float32),
        "fs",
        scatter_dimension=0,
        tiled=True,
    )
    partial_diff = jnp.dot(gate_diff, gate_whole.T, preferred_element_type=jnp.float32)
    partial_diff = partial_diff + jnp.dot(up_diff, up_whole.T, preferred_element_type=jnp.float32)
    normed_diff = lax.psum(partial_diff.astype(jnp.bfloat16), "tp").astype(jnp.float32)
    scaled = normed_diff * norm_gain
    cubed = factor * factor * factor
    back_grad = (
        factor * scaled - values * cubed * jnp.mean(scaled * values, axis=-1, keepdims=True)
    ).astype(jnp.bfloat16)
    back_grad, gate_grad_out = (back_grad, gate_grad_out)
    return (fwd_out, back_grad, gate_grad_out)


MESH = pl.DeviceIdType.MESH


def wide_dot(a, b):
    return lax.dot_general(a, b, (((1,), (1,)), ((), ())), preferred_element_type=jnp.float32)


def padded(size):
    return (size + 127) // 128 * 128


def layer_kernel(
    split, fwd_ref, tokens_ref, grad_ref, gain_ref, gate_ref, up_ref, down_ref, sum_ref,
    fwd_out, back_out, sum_out,
    turned, normed, toks, weights, staged, back_acc, down_acc, fwd_acc, hidden, diffs, diff_cols,
    early, part, crossed, joined, folded, gathered, grad_send, grad_side, grad_total, grad_pass, grad_recv, grad_turn, turn_recv, grad_cols,
    stage_send, stage_recv, weight_recv, far_send, near_send, other_send, pass_send, side_send,
    tok_send, tok_recv, relay_send, relay_recv, gside_send, gside_recv, glev_send, glev_recv,
    gpass_send, gpass_recv, gturn_send, gturn_recv,
    cross_sem, join_send, join_recv, last_sem,
):
    fs, core = lax.axis_index("fs"), lax.axis_index("tp")
    x, y, z = fs % 2, fs // 2 % 2, fs // 4
    odd = z % 2
    inner = jnp.logical_and(z > 0, z < 3)
    near, far, other = z + 1 - 2 * odd, (z + 2) % 4, 3 - z
    sibling = (fs, 1 - core)
    rows = turned.shape[1] // 4
    starts, sizes = (0, split), (split, rows - split)
    pads = tuple(padded(size) for size in sizes)
    depth = gate_ref.shape[0]
    half = fwd_ref.shape[0] // 2
    slab = half * 4
    width = fwd_ref.shape[1]
    band = 4 * depth

    def chip(to_x, to_y, to_z):
        return (to_z * 4 + to_y * 2 + to_x, core)

    beside, across = chip(1 - x, y, z), chip(x, 1 - y, z)
    y_flip = 1 - y

    barrier = pltpu.get_barrier_semaphore()
    for device in (
        sibling, beside, across, chip(x, y, near), chip(x, y, far), chip(x, y, other),
        chip(x, 1 - y, near), chip(x, 1 - y, far), chip(x, 1 - y, other),
    ):
        pl.semaphore_signal(barrier, inc=1, device_id=device, device_id_type=MESH)

    @pl.loop(0, turned.shape[1] // 128)
    def _(t):
        at = pl.ds(pl.multiple_of(t * 128, 128), 128)
        turned[0, at, :] = gate_ref[:, at].T
        turned[1, at, :] = up_ref[:, at].T
        turned[2, at, :] = down_ref[:, at].T

    pl.semaphore_wait(barrier, 9)

    def remote(src, dst, send, recv, device):
        return pltpu.make_async_remote_copy(
            src_ref=src, dst_ref=dst, send_sem=send, recv_sem=recv, device_id=device, device_id_type=MESH
        )

    def own_rows(h, to_y, to_odd):
        return pl.ds(pl.multiple_of((to_y * 2 + to_odd) * rows + starts[h], 16), sizes[h])

    def held_rows(w, h):
        return pl.ds(3 * starts[h] + w * pads[h], sizes[h])

    def both_rows(w, h, count=1):
        return pl.ds(3 * starts[h] + w * pads[h], count * pads[h])

    def own(w, h, to_y, to_odd):
        return turned.at[w, own_rows(h, to_y, to_odd), :]

    def lanes(src):
        return pl.ds(pl.multiple_of(src * depth, depth), depth)

    def level_lanes(s):
        return pl.ds(pl.multiple_of(s * band, band), band)

    def block(w, h, src):
        return weights.at[held_rows(w, h), lanes(src)]

    def send_block(w, h, src, source, sem, device):
        return remote(source, block(w, h, src), sem, weight_recv.at[w, h, src], device)

    def block_in(w, h, src):
        send_block(w, h, src, block(w, h, src), stage_send.at[w, h, 0], sibling).wait_recv()

    def side(w, h, src, source):
        return send_block(w, h, src, source, side_send.at[w, h, src // 2], beside)

    def held(w, h):
        return remote(own(w, h, 1 - y, 1 - odd), staged.at[held_rows(w, h), :], stage_send.at[w, h, 1], stage_recv.at[w, h], across)

    def send_own(h):
        for w in range(3):
            send_block(w, h, fs, own(w, h, 1 - y, odd), stage_send.at[w, h, 0], across).start()
            held(w, h).start()
            send_block(w, h, fs, own(w, h, y, 1 - odd), near_send.at[w, h, 0], chip(x, y, near)).start()
            send_block(w, h, fs, own(w, h, y, odd), far_send.at[w, h, 0], chip(x, y, far)).start()

            @pl.when(inner)
            def _():
                send_block(w, h, fs, own(w, h, y, 1 - odd), other_send.at[w, h, 0], chip(x, y, other)).start()

            side(w, h, fs, own(w, h, y, odd)).start()

    def keep_own(h):
        for w in range(3):
            weights[held_rows(w, h), lanes(fs)] = turned[w, own_rows(h, y, odd), :]

    def clear_pads():
        for h in range(2):
            if pads[h] > sizes[h]:
                for w in range(3):
                    gap = pl.ds(3 * starts[h] + w * pads[h] + sizes[h], pads[h] - sizes[h])
                    weights[gap, :] = jnp.zeros((pads[h] - sizes[h], width), jnp.bfloat16)

    def stage_in(w, h):
        src = z * 4 + (1 - y) * 2 + x
        held(w, h).wait_recv()
        send_block(w, h, src, staged.at[held_rows(w, h), :], near_send.at[w, h, 1], chip(x, y, near)).start()

        @pl.when(inner)
        def _():
            send_block(w, h, src, staged.at[held_rows(w, h), :], other_send.at[w, h, 1], chip(x, y, other)).start()

        block_in(w, h, src)
        send_block(w, h, src, block(w, h, src), far_send.at[w, h, 1], chip(x, y, far)).start()
        side(w, h, src, block(w, h, src)).start()

    def line_in(h, s, line):
        for w in range(3):
            src = s * 4 + line * 2 + x
            block_in(w, h, src)
            if s is near:

                @pl.when(inner)
                def _():
                    send_block(w, h, src, block(w, h, src), pass_send.at[w, h, int(line is not y)], chip(x, y, far)).start()

            side(w, h, src, block(w, h, src)).start()

    def side_in(w, h, s):
        for line in range(2):
            block_in(w, h, s * 4 + line * 2 + 1 - x)

    me = y * 2 + odd
    at_near, at_across, at_both = y * 2 + 1 - odd, (1 - y) * 2 + odd, (1 - y) * 2 + 1 - odd

    def token_rows(a, at):
        return grad_ref.at[at, :] if a == 2 else normed.at[a, at, :]

    def tok_block(a, h, q):
        return toks.at[a, pl.ds(pl.multiple_of(h * slab + q * half, half), half), :]

    def tok_copy(a, n, q, source, device):
        return remote(source, tok_block(a, core, q), tok_send.at[a, n], tok_recv.at[a, q], device)

    def relay(a, q):
        return remote(tok_block(a, core, q), tok_block(a, core, q), relay_send.at[a, q], relay_recv.at[a, q], sibling)

    def send_tokens(a, n):
        mine = token_rows(a, pl.ds(pl.multiple_of(core * half, half), half))
        tok_copy(a, n, me, mine, (chip(x, y, near), across)[n]).start()

    def normal(a):
        @pl.loop(0, tokens_ref.shape[0] // 16)
        def _(r):
            at = pl.ds(pl.multiple_of(r * 16, 16), 16)
            normed[a, at, :] = normalize((tokens_ref, fwd_ref)[a][at, :], gain_ref[...])[2]

    def keep_tokens(a):
        for h in range(2):
            toks[a, pl.ds(pl.multiple_of(h * slab + me * half, half), half), :] = token_rows(a, pl.ds(h * half, half))[...]

    def tok_in(a, q):
        tok_copy(a, 0, q, tok_block(a, core, q), sibling).wait_recv()
        if q is at_near:
            tok_copy(a, 2, q, tok_block(a, core, q), across).start()
        relay(a, q).start()

    def relayed(a):
        for q in (at_near, at_across, at_both):
            remote(tok_block(a, 1 - core, q), tok_block(a, 1 - core, q), relay_send.at[a, q], relay_recv.at[a, q], sibling).wait_recv()

    def project(h, kind, levels, first=True):
        a, w, count, into = ((0, 0, 2, back_acc), (2, 2, 1, down_acc), (1, 0, 2, fwd_acc))[kind]
        wide = count * pads[h]
        at_rows = both_rows(w, h, count)
        for t in range(2):
            at_tokens = pl.ds(t * slab, slab)
            value = None if first else into[h, at_tokens, :wide]
            for s in levels:
                at = level_lanes(s)
                term = wide_dot(toks[a, at_tokens, at], weights[at_rows, at])
                value = term if value is None else value + term
            into[h, at_tokens, :wide] = value

    piece = 64

    def back_parts(h):
        n = pads[h]

        @pl.loop(0, 2 * slab // piece)
        def _(r):
            at = pl.ds(pl.multiple_of(r * piece, piece), piece)
            gate, up = back_acc[h, at, :n], back_acc[h, at, n : 2 * n]
            s = jax.nn.sigmoid(gate)
            back = 0.5 * down_acc[h, at, :n]
            gate_diff = (back * up * s * (1.0 + gate * (1.0 - s))).astype(jnp.bfloat16)
            diff_cols[h, at, :n] = gate_diff
            diffs[h, at, :n] = gate_diff
            diffs[h, at, n : 2 * n] = (back * gate * s).astype(jnp.bfloat16)

    def fwd_parts(h):
        n = pads[h]

        @pl.loop(0, 2 * slab // piece)
        def _(r):
            at = pl.ds(pl.multiple_of(r * piece, piece), piece)
            gate, up = fwd_acc[h, at, :n], fwd_acc[h, at, n : 2 * n]
            hidden[h, at, :n] = (gate * jax.nn.sigmoid(gate) * up).astype(jnp.bfloat16)

    def grad_rows(h):
        return pl.ds(starts[h], sizes[h])

    def grad_across(h, n):
        pair = pl.ds((other, far, near, z)[n] * 2, 2)
        return remote(
            grad_send.at[1 - x, pair, grad_rows(h)], grad_side.at[pair, grad_rows(h)], gside_send.at[h, n], gside_recv.at[h, n], beside
        )

    def grad_make(h):
        diff_turned = diff_cols[h, :, : sizes[h]].T
        for s in range(4):
            at = level_lanes(s)
            product = jnp.dot(diff_turned, toks[0, :, at], preferred_element_type=jnp.float32)
            product = product.astype(jnp.bfloat16)
            for q in range(4):
                grad_send[q % 2, s * 2 + q // 2, grad_rows(h), :] = product[:, q * depth : (q + 1) * depth]

    def grad_out(h):
        for s in range(4):
            grad_across(h, s).start()

    def grad_to(h, n):
        s = (near, far, other)[n]
        source = grad_total.at[pl.ds(s * 2, 2), grad_rows(h)]
        return remote(source, grad_recv.at[n, :, grad_rows(h)], glev_send.at[h, n], glev_recv.at[h, n], chip(x, y, s))

    def grad_past(h):
        source = grad_total.at[pl.ds(other * 2, 2), grad_rows(h)]
        return remote(source, grad_pass.at[:, grad_rows(h)], gpass_send.at[h], gpass_recv.at[h], chip(x, y, far))

    def grad_turned(h):
        return remote(
            grad_turn.at[:, grad_rows(h)], turn_recv.at[:, grad_rows(h)], gturn_send.at[h], gturn_recv.at[h], across
        )

    def grad_on(h, n):
        grad_across(h, n).wait_recv()
        for line in range(2):
            j = (other, far, near, z)[n] * 2 + line
            total = grad_send[x, j, grad_rows(h), :].astype(jnp.float32) + grad_side[j, grad_rows(h), :].astype(jnp.float32)
            grad_total[j, grad_rows(h), :] = total.astype(jnp.bfloat16)
        if n == 0:

            @pl.when(inner)
            def _():
                grad_to(h, 2).start()

            @pl.when(jnp.logical_not(inner))
            def _():
                grad_past(h).start()

        if n == 1:
            grad_to(h, 1).start()
        if n == 2:

            @pl.when(jnp.logical_not(inner))
            def _():
                grad_to(h, 0).start()

    def grad_mid(h):
        @pl.when(inner)
        def _():
            grad_past(h).wait_recv()
            for line in range(2):
                j = near * 2 + line
                total = grad_total[j, grad_rows(h), :].astype(jnp.float32) + grad_pass[line, grad_rows(h), :].astype(jnp.float32)
                grad_total[j, grad_rows(h), :] = total.astype(jnp.bfloat16)
            grad_to(h, 0).start()

    def grad_cols_at(h, to_y, to_odd):
        return pl.ds(pl.multiple_of((to_y * 2 + to_odd) * rows + starts[h], 16), sizes[h])

    def grad_cross(h):
        at = grad_rows(h)
        for n in range(2):
            grad_to(h, n).wait_recv()

        @pl.when(inner)
        def _():
            grad_to(h, 2).wait_recv()
            for line in range(2):
                total = grad_recv[0, line, at, :].astype(jnp.float32) + grad_recv[2, line, at, :].astype(jnp.float32)
                grad_recv[0, line, at, :] = total.astype(jnp.bfloat16)

        def sums(line):
            same = grad_total[z * 2 + line, at, :].astype(jnp.float32) + grad_recv[1, line, at, :].astype(jnp.float32)
            return same, grad_recv[0, line, at, :]

        same, unlike = sums(1 - y)
        grad_turn[0, at, :] = same.astype(jnp.bfloat16)
        grad_turn[1, at, :] = unlike
        grad_turned(h).start()
        same, unlike = sums(y)
        grad_cols[grad_cols_at(h, y, odd), :] = same
        grad_cols[grad_cols_at(h, y, 1 - odd), :] = unlike.astype(jnp.float32)

    def grad_in(h):
        grad_turned(h).wait_recv()
        for n, to_odd in enumerate((odd, 1 - odd)):
            grad_cols[grad_cols_at(h, 1 - y, to_odd), :] = turn_recv[n, grad_rows(h), :].astype(jnp.float32)

    span = width // 2

    def columns(c):
        return pl.ds(c * span, span)

    def cross(k, c):
        at = columns(c)
        return remote(
            part.at[k, 1 - core, :, at], crossed.at[k, :, at], cross_sem.at[k, c, 0], cross_sem.at[k, c, 1], sibling
        )

    strip = 512

    def product_of(k, h, rows_at, at):
        n = pads[h]
        if k == 0:
            return jnp.dot(hidden[h, rows_at, :n], weights[both_rows(2, h), at], preferred_element_type=jnp.float32)
        return jnp.dot(diffs[h, rows_at, : 2 * n], weights[both_rows(0, h, 2), at], preferred_element_type=jnp.float32)

    def partial_early(k):
        @pl.loop(0, width // strip)
        def _(c):
            at = pl.ds(pl.multiple_of(c * strip, strip), strip)
            early[k, :, at] = product_of(k, 0, slice(None), at)

    def partial(k, t, c):
        rows_at = pl.ds(pl.multiple_of(t * slab, slab), slab)
        at = columns(c)
        part[k, t, :, at] = (early[k, rows_at, at] + product_of(k, 1, rows_at, at)).astype(jnp.bfloat16)

    routes = ((across, at_across, at_near, chip(x, y, near)), (chip(x, y, near), at_near, at_across, across))
    routed = ((0, 0), (1, 0))
    def join_copy(k, c, n):
        to, theirs, mine, on = routes[routed[k][c]]
        at = columns(c)
        if n == 2:
            source, device = folded.at[k, :, at], on
        else:
            source, device = joined.at[k, (at_both, theirs)[n], :, at], to
        return remote(source, gathered.at[k, n, :, at], join_send.at[k, c, n], join_recv.at[k, c, n], device)

    def join_start(k, c):
        cross(k, c).wait_recv()
        at = columns(c)
        for n, q in enumerate((at_both, *routes[routed[k][c]][1:3], me)):
            rows_at = pl.ds(pl.multiple_of(q * half, half), half)
            total = part[k, core, rows_at, at].astype(jnp.float32) + crossed[k, rows_at, at].astype(jnp.float32)
            joined[k, q, :, at] = total.astype(jnp.bfloat16)
            if n < 2:
                join_copy(k, c, n).start()

    def join_fold(k, c):
        at = columns(c)
        join_copy(k, c, 0).wait_recv()
        total = gathered[k, 0, :, at].astype(jnp.float32) + joined[k, routes[routed[k][c]][2], :, at].astype(jnp.float32)
        folded[k, :, at] = total.astype(jnp.bfloat16)
        join_copy(k, c, 2).start()

    levels = (z, near, far, other)

    def sides_in(h, some):
        for w in range(3):
            for s in some:
                side_in(w, h, s)

    def stages_in(h):
        for w in range(3):
            stage_in(w, h)

    send_own(0)
    send_own(1)
    send_tokens(2, 1)
    normal(0)
    send_tokens(0, 1)
    normal(1)
    send_tokens(1, 1)
    clear_pads()
    for h in range(2):
        keep_own(h)
    for a in range(3):
        keep_tokens(a)
    stages_in(0)
    send_tokens(2, 0)
    send_tokens(0, 0)
    send_tokens(1, 0)
    stages_in(1)
    for h in range(2):
        line_in(h, near, y)
        line_in(h, far, y)
    tok_in(2, at_across)
    line_in(0, near, y_flip)
    line_in(0, far, y_flip)
    tok_in(2, at_near)
    tok_in(0, at_across)
    line_in(0, other, y)
    line_in(1, far, y_flip)
    tok_in(0, at_near)
    line_in(1, other, y)
    tok_in(1, at_across)
    tok_in(2, at_both)
    line_in(0, other, y_flip)
    line_in(1, near, y_flip)
    tok_in(0, at_both)
    relayed(2)
    sides_in(0, levels)
    tok_in(1, at_near)
    project(0, 1, levels)
    relayed(0)
    line_in(1, other, y_flip)
    project(0, 0, levels)
    back_parts(0)
    grad_make(0)
    grad_out(0)
    partial_early(1)
    sides_in(1, levels[:3])
    for kind in range(2):
        project(1, kind, levels[:3])
    tok_in(1, at_both)
    relayed(1)
    project(0, 2, levels)
    fwd_parts(0)
    partial_early(0)
    project(1, 2, levels[:3])
    sides_in(1, levels[3:])
    project(1, 0, levels[3:], False)
    project(1, 1, levels[3:], False)
    back_parts(1)
    for c in range(2):
        partial(1, 1 - core, c)
        cross(1, c).start()
    for c in range(2):
        partial(1, core, c)
        join_start(1, c)
    project(1, 2, levels[3:], False)
    fwd_parts(1)
    for c in range(2):
        partial(0, 1 - core, c)
        cross(0, c).start()
    for c in range(2):
        partial(0, core, c)
        join_start(0, c)
    grad_make(1)
    grad_out(1)
    for n in range(4):
        grad_on(0, n)
    for c in range(2):
        join_fold(1, c)
    grad_mid(0)
    for n in range(4):
        grad_on(1, n)
    for c in range(2):
        join_fold(0, c)
    grad_mid(1)
    grad_cross(0)
    grad_cross(1)

    mine = pl.ds(pl.multiple_of(core * half, half), half)

    def last(k):
        out = (fwd_out, back_out)[k]
        return remote(out.at[mine, :], out.at[mine, :], last_sem.at[k, 0], last_sem.at[k, 1], sibling)

    def joined_in(k):
        for c in range(2):
            for n in (1, 2):
                join_copy(k, c, n).wait_recv()

    def total_of(k, at):
        value = joined[k, me, at, :].astype(jnp.float32) + gathered[k, 1, at, :].astype(jnp.float32)
        return value + gathered[k, 2, at, :].astype(jnp.float32)

    small = 16
    joined_in(0)
    for r in range(half // small):
        at = pl.ds(r * small, small)
        fwd_out[pl.ds(pl.multiple_of(core * half + r * small, small), small), :] = (0.5 * total_of(0, at)).astype(jnp.bfloat16)
    last(0).start()
    joined_in(1)
    for r in range(half // small):
        at = pl.ds(r * small, small)
        there = pl.ds(pl.multiple_of(core * half + r * small, small), small)
        values = tokens_ref[there, :].astype(jnp.float32)
        factor = lax.rsqrt(jnp.mean(values * values, axis=-1, keepdims=True) + norm_eps)
        scaled = total_of(1, at) * gain_ref[...]
        cubed = factor * factor * factor
        back_out[there, :] = (
            factor * scaled - values * cubed * jnp.mean(scaled * values, axis=-1, keepdims=True)
        ).astype(jnp.bfloat16)
    last(1).start()

    for h in range(2):
        grad_in(h)

    @pl.loop(0, grad_cols.shape[0] // 128)
    def _(t):
        at = pl.ds(pl.multiple_of(t * 128, 128), 128)
        sum_out[:, at] = sum_ref[:, at] + grad_cols[at, :].T

    for h in range(2):
        for w in range(3):
            for n in range(2):
                gone = block(w, h, fs)
                for sem in (stage_send, near_send, far_send):
                    send_block(w, h, fs, gone, sem.at[w, h, n], sibling).wait_send()

                @pl.when(inner)
                def _():
                    for sem in (other_send, pass_send):
                        send_block(w, h, fs, gone, sem.at[w, h, n], sibling).wait_send()

            @pl.loop(0, 8)
            def _(j):
                send_block(w, h, fs, gone, side_send.at[w, h, j], sibling).wait_send()

        for s in range(4):
            grad_across(h, s).wait_send()
        grad_to(h, 0).wait_send()
        grad_to(h, 1).wait_send()
        grad_turned(h).wait_send()

        @pl.when(inner)
        def _():
            grad_to(h, 2).wait_send()

        @pl.when(jnp.logical_not(inner))
        def _():
            grad_past(h).wait_send()

    for a in range(3):
        for n in range(3):
            tok_copy(a, n, me, tok_block(a, core, me), sibling).wait_send()
        for q in (at_near, at_across, at_both):
            relay(a, q).wait_send()
    for k in range(2):
        for c in range(2):
            cross(k, c).wait_send()
            for n in range(3):
                join_copy(k, c, n).wait_send()
        last(k).wait()


def fused_shards(
    split, fwd_tokens, back_tokens, out_grad, norm_gain, gate_weight, up_weight, down_weight, gate_grad_sum
):
    tokens, width = fwd_tokens.shape
    depth, cols = gate_weight.shape
    rows = cols // 4
    wide = max(padded(split), padded(rows - split))
    held = 3 * (padded(split) + padded(rows - split))
    half = tokens // 2
    slab = half * 4
    narrow, full = jnp.bfloat16, jnp.float32
    dma = pltpu.SemaphoreType.DMA
    vmem = pl.BlockSpec(memory_space=pltpu.VMEM)
    return pl.pallas_call(
        functools.partial(layer_kernel, split),
        out_shape=(
            jax.ShapeDtypeStruct((tokens, width), narrow),
            jax.ShapeDtypeStruct((tokens, width), narrow),
            jax.ShapeDtypeStruct((depth, cols), full),
        ),
        in_specs=[vmem] * 8,
        out_specs=(vmem,) * 3,
        scratch_shapes=[
            pltpu.VMEM((3, cols, depth), narrow),
            pltpu.VMEM((2, tokens, width), narrow),
            pltpu.VMEM((3, 2 * slab, width), narrow),
            pltpu.VMEM((held, width), narrow),
            pltpu.VMEM((held, depth), narrow),
            pltpu.VMEM((2, 2 * slab, 2 * wide), full),
            pltpu.VMEM((2, 2 * slab, wide), full),
            pltpu.VMEM((2, 2 * slab, 2 * wide), full),
            pltpu.VMEM((2, 2 * slab, wide), narrow),
            pltpu.VMEM((2, 2 * slab, 2 * wide), narrow),
            pltpu.VMEM((2, 2 * slab, wide), narrow),
            pltpu.VMEM((2, 2 * slab, width), full),
            pltpu.VMEM((2, 2, slab, width), narrow),
            pltpu.VMEM((2, slab, width), narrow),
            pltpu.VMEM((2, 4, half, width), narrow),
            pltpu.VMEM((2, half, width), narrow),
            pltpu.VMEM((2, 3, half, width), narrow),
            pltpu.VMEM((2, 8, rows, depth), narrow),
            pltpu.VMEM((8, rows, depth), narrow),
            pltpu.VMEM((8, rows, depth), narrow),
            pltpu.VMEM((2, rows, depth), narrow),
            pltpu.VMEM((3, 2, rows, depth), narrow),
            pltpu.VMEM((2, rows, depth), narrow),
            pltpu.VMEM((2, rows, depth), narrow),
            pltpu.VMEM((cols, depth), full),
            dma((3, 2, 2)),
            dma((3, 2)),
            dma((3, 2, 16)),
            dma((3, 2, 2)),
            dma((3, 2, 2)),
            dma((3, 2, 2)),
            dma((3, 2, 2)),
            dma((3, 2, 8)),
            dma((3, 3)),
            dma((3, 4)),
            dma((3, 4)),
            dma((3, 4)),
            dma((2, 4)),
            dma((2, 4)),
            dma((2, 3)),
            dma((2, 3)),
            dma((2,)),
            dma((2,)),
            dma((2,)),
            dma((2,)),
            dma((2, 2, 2)),
            dma((2, 2, 3)),
            dma((2, 2, 3)),
            dma((2, 2)),
        ],
        compiler_params=pltpu.CompilerParams(
            collective_id=0, has_side_effects=True, vmem_limit_bytes=60 * 2**20
        ),
    )(
        fwd_tokens, back_tokens, out_grad, norm_gain.reshape(1, width),
        gate_weight, up_weight, down_weight, gate_grad_sum,
    )


def body_for(mesh):
    def body(*args):
        tokens, width = args[0].shape
        depth, cols = args[4].shape
        rows = cols // 4
        fits = (
            mesh.shape["tp"] == 2 and mesh.shape["fs"] == 16
            and depth == 128 and width == 16 * depth and cols % 128 == 0 and tokens % 128 == 0
            and rows > 256 and rows % 16 == 0
        )
        if not fits:
            return shards(*args)
        return fused_shards((rows - 1) // 256 * 256, *args)

    return body


def solution(mesh):
    in_specs = (
        P("fs", None),
        P("fs", None),
        P("fs", None),
        P(),
        P("fs", "tp"),
        P("fs", "tp"),
        P("fs", "tp"),
        P("fs", "tp"),
    )
    out_specs = (P("fs", None), P("fs", None), P("fs", "tp"))
    return jax.shard_map(body_for(mesh), mesh=mesh, in_specs=in_specs, out_specs=out_specs, check_vma=False)
```

```python
import functools

import jax
import jax.numpy as jnp
from jax import lax
from jax.experimental import pallas as pl
from jax.experimental.pallas import tpu as pltpu
from jax.sharding import PartitionSpec as P

norm_eps = 0.25
vmem_bytes = 66_900_000


def normalize(tokens, norm_gain):
    values = tokens.astype(jnp.float32)
    factor = lax.rsqrt(jnp.mean(values * values, axis=-1, keepdims=True) + norm_eps)
    return (values, factor, (values * factor * norm_gain).astype(jnp.bfloat16))


def shards(
    fwd_tokens, back_tokens, out_grad, norm_gain, gate_weight, up_weight, down_weight, gate_grad_sum
):
    fwd_normed = normalize(fwd_tokens, norm_gain)[2]
    columns = fwd_normed
    gate_pre = jnp.dot(
        columns,
        lax.all_gather(gate_weight, "fs", axis=0, tiled=True),
        preferred_element_type=jnp.float32,
    )
    up_pre = jnp.dot(
        columns,
        lax.all_gather(up_weight, "fs", axis=0, tiled=True),
        preferred_element_type=jnp.float32,
    )
    hidden = (gate_pre * jax.nn.sigmoid(gate_pre) * up_pre).astype(jnp.bfloat16)
    partial_value = jnp.dot(
        hidden,
        lax.all_gather(down_weight, "fs", axis=0, tiled=True).T,
        preferred_element_type=jnp.float32,
    )
    summed = lax.psum(partial_value.astype(jnp.bfloat16), "tp").astype(jnp.float32)
    fwd_out = (0.5 * summed).astype(jnp.bfloat16)
    gate_whole = lax.all_gather(gate_weight, "fs", axis=0, tiled=True)
    up_whole = lax.all_gather(up_weight, "fs", axis=0, tiled=True)
    down_whole = lax.all_gather(down_weight, "fs", axis=0, tiled=True)
    values, factor, back_normed = normalize(back_tokens, norm_gain)
    gate_pre = jnp.dot(back_normed, gate_whole, preferred_element_type=jnp.float32)
    up_pre = jnp.dot(back_normed, up_whole, preferred_element_type=jnp.float32)
    sigmoid_gate = jax.nn.sigmoid(gate_pre)
    back_hidden = 0.5 * jnp.dot(out_grad, down_whole, preferred_element_type=jnp.float32)
    gate_diff = (
        back_hidden * up_pre * sigmoid_gate * (1.0 + gate_pre * (1.0 - sigmoid_gate))
    ).astype(jnp.bfloat16)
    up_diff = (back_hidden * gate_pre * sigmoid_gate).astype(jnp.bfloat16)
    columns = back_normed
    gate_grad_out = gate_grad_sum + lax.psum_scatter(
        jnp.dot(columns.T, gate_diff, preferred_element_type=jnp.float32),
        "fs",
        scatter_dimension=0,
        tiled=True,
    )
    partial_diff = jnp.dot(gate_diff, gate_whole.T, preferred_element_type=jnp.float32)
    partial_diff = partial_diff + jnp.dot(up_diff, up_whole.T, preferred_element_type=jnp.float32)
    normed_diff = lax.psum(partial_diff.astype(jnp.bfloat16), "tp").astype(jnp.float32)
    scaled = normed_diff * norm_gain
    cubed = factor * factor * factor
    back_grad = (
        factor * scaled - values * cubed * jnp.mean(scaled * values, axis=-1, keepdims=True)
    ).astype(jnp.bfloat16)
    back_grad, gate_grad_out = (back_grad, gate_grad_out)
    return (fwd_out, back_grad, gate_grad_out)


MESH = pl.DeviceIdType.MESH


def wide_dot(a, b):
    return lax.dot_general(a, b, (((1,), (1,)), ((), ())), preferred_element_type=jnp.float32)


def padded(size):
    return (size + 127) // 128 * 128


def layer_kernel(
    split, fwd_in, tokens_in, grad_in_ref, gain_ref, gate_in, up_in, down_in, sum_in,
    fwd_out, back_out, sum_out,
    raw, raw_tokens, sum_ref, turned, normed, toks, weights, staged, back_acc, down_acc, fwd_acc, hidden, diffs, diff_cols,
    part, crossed, joined, folded, gathered, grad_send, grad_side, grad_total, grad_pass, grad_recv, grad_turn, turn_recv, grad_cols,
    stage_send, stage_recv, weight_recv, far_send, near_send, other_send, pass_send, side_send,
    tok_send, tok_recv, relay_send, relay_recv, gside_send, gside_recv, glev_send, glev_recv,
    gpass_send, gpass_recv, gturn_send, gturn_recv,
    cross_sem, join_send, join_recv, last_sem, raw_sem, token_sem, sum_sem,
):
    fs, core = lax.axis_index("fs"), lax.axis_index("tp")
    x, y, z = fs % 2, fs // 2 % 2, fs // 4
    odd = z % 2
    inner = jnp.logical_and(z > 0, z < 3)
    near, far, other = z + 1 - 2 * odd, (z + 2) % 4, 3 - z
    sibling = (fs, 1 - core)
    rows = turned.shape[1] // 4
    starts, sizes = (0, split), (split, rows - split)
    pads = tuple(padded(size) for size in sizes)
    depth = gate_in.shape[0]
    half = fwd_in.shape[0] // 2
    tokens_ref, fwd_ref, grad_ref = raw_tokens.at[0], raw_tokens.at[1], raw_tokens.at[2]
    slab = half * 4
    width = fwd_in.shape[1]
    band = 4 * depth

    def chip(to_x, to_y, to_z):
        return (to_z * 4 + to_y * 2 + to_x, core)

    beside, across = chip(1 - x, y, z), chip(x, 1 - y, z)
    y_flip = 1 - y

    barrier = pltpu.get_barrier_semaphore()
    for device in (
        sibling, beside, across, chip(x, y, near), chip(x, y, far), chip(x, y, other),
        chip(x, 1 - y, near), chip(x, 1 - y, far), chip(x, 1 - y, other),
    ):
        pl.semaphore_signal(barrier, inc=1, device_id=device, device_id_type=MESH)

    raw_copies = [pltpu.make_async_copy(ref, raw.at[w], raw_sem.at[w]) for w, ref in enumerate((gate_in, up_in, down_in))]
    token_copies = [
        pltpu.make_async_copy(ref, raw_tokens.at[a], token_sem.at[a]) for a, ref in enumerate((tokens_in, fwd_in, grad_in_ref))
    ]
    sum_copy = pltpu.make_async_copy(sum_in, sum_ref, sum_sem.at[0])
    for copy in (*raw_copies, token_copies[2], token_copies[0], token_copies[1], sum_copy):
        copy.start()

    def turn_in(w):
        raw_copies[w].wait()
        for n in range(turned.shape[1] // 128):
            at = pl.ds(n * 128, 128)
            turned[w, at, :] = raw[w, :, at].T

    def remote(src, dst, send, recv, device):
        return pltpu.make_async_remote_copy(
            src_ref=src, dst_ref=dst, send_sem=send, recv_sem=recv, device_id=device, device_id_type=MESH
        )

    def own_rows(h, to_y, to_odd):
        return pl.ds(pl.multiple_of((to_y * 2 + to_odd) * rows + starts[h], 16), sizes[h])

    def held_rows(w, h):
        return pl.ds(3 * starts[h] + w * pads[h], sizes[h])

    def both_rows(w, h, count=1):
        return pl.ds(3 * starts[h] + w * pads[h], count * pads[h])

    def own(w, h, to_y, to_odd):
        return turned.at[w, own_rows(h, to_y, to_odd), :]

    def lanes(src):
        return pl.ds(pl.multiple_of(src * depth, depth), depth)

    def level_lanes(s):
        return pl.ds(pl.multiple_of(s * band, band), band)

    def block(w, h, src):
        return weights.at[held_rows(w, h), lanes(src)]

    def send_block(w, h, src, source, sem, device):
        return remote(source, block(w, h, src), sem, weight_recv.at[w, h, src], device)

    def block_in(w, h, src):
        send_block(w, h, src, block(w, h, src), stage_send.at[w, h, 0], sibling).wait_recv()

    def side(w, h, src, source):
        return send_block(w, h, src, source, side_send.at[w, h, src // 2], beside)

    def held(w, h):
        return remote(own(w, h, 1 - y, 1 - odd), staged.at[held_rows(w, h), :], stage_send.at[w, h, 1], stage_recv.at[w, h], across)

    def send_stage(h, some=range(3)):
        for w in some:
            send_block(w, h, fs, own(w, h, 1 - y, odd), stage_send.at[w, h, 0], across).start()
            held(w, h).start()

    def send_own(h, some=range(3)):
        for w in some:
            send_block(w, h, fs, own(w, h, y, 1 - odd), near_send.at[w, h, 0], chip(x, y, near)).start()
            send_block(w, h, fs, own(w, h, y, odd), far_send.at[w, h, 0], chip(x, y, far)).start()

            @pl.when(inner)
            def _():
                send_block(w, h, fs, own(w, h, y, 1 - odd), other_send.at[w, h, 0], chip(x, y, other)).start()

            side(w, h, fs, own(w, h, y, odd)).start()

    def keep_own(h):
        for w in range(3):
            weights[held_rows(w, h), lanes(fs)] = turned[w, own_rows(h, y, odd), :]

    def clear_pads():
        for h in range(2):
            if pads[h] > sizes[h]:
                for w in range(3):
                    gap = pl.ds(3 * starts[h] + w * pads[h] + sizes[h], pads[h] - sizes[h])
                    weights[gap, :] = jnp.zeros((pads[h] - sizes[h], width), jnp.bfloat16)

    def stage_in(w, h):
        src = z * 4 + (1 - y) * 2 + x
        held(w, h).wait_recv()
        send_block(w, h, src, staged.at[held_rows(w, h), :], near_send.at[w, h, 1], chip(x, y, near)).start()

        @pl.when(inner)
        def _():
            send_block(w, h, src, staged.at[held_rows(w, h), :], other_send.at[w, h, 1], chip(x, y, other)).start()

        block_in(w, h, src)
        send_block(w, h, src, block(w, h, src), far_send.at[w, h, 1], chip(x, y, far)).start()
        side(w, h, src, block(w, h, src)).start()

    def line_in(h, s, line):
        for w in range(3):
            src = s * 4 + line * 2 + x
            block_in(w, h, src)
            if s is near:

                @pl.when(inner)
                def _():
                    send_block(w, h, src, block(w, h, src), pass_send.at[w, h, int(line is not y)], chip(x, y, far)).start()

            side(w, h, src, block(w, h, src)).start()

    def sides_in(h, groups):
        for w in range(3):
            for s, line in groups:
                block_in(w, h, s * 4 + line * 2 + 1 - x)

    me = y * 2 + odd
    at_near, at_across, at_both = y * 2 + 1 - odd, (1 - y) * 2 + odd, (1 - y) * 2 + 1 - odd

    def token_rows(a, at):
        return grad_ref.at[at, :] if a == 2 else normed.at[a, at, :]

    def tok_block(a, h, q):
        return toks.at[a, pl.ds(pl.multiple_of(h * slab + q * half, half), half), :]

    def tok_copy(a, n, q, source, device):
        return remote(source, tok_block(a, core, q), tok_send.at[a, n], tok_recv.at[a, q], device)

    def relay(a, q):
        return remote(tok_block(a, core, q), tok_block(a, core, q), relay_send.at[a, q], relay_recv.at[a, q], sibling)

    def send_tokens(a, n):
        mine = token_rows(a, pl.ds(pl.multiple_of(core * half, half), half))
        tok_copy(a, n, me, mine, (chip(x, y, near), across)[n]).start()

    def normal(a):
        @pl.loop(0, tokens_ref.shape[0] // 16)
        def _(r):
            at = pl.ds(pl.multiple_of(r * 16, 16), 16)
            normed[a, at, :] = normalize((tokens_ref, fwd_ref)[a][at, :], gain_ref[...])[2]

    def keep_tokens(a):
        for h in range(2):
            toks[a, pl.ds(pl.multiple_of(h * slab + me * half, half), half), :] = token_rows(a, pl.ds(h * half, half))[...]

    def tok_in(a, q):
        tok_copy(a, 0, q, tok_block(a, core, q), sibling).wait_recv()
        if q is at_near:
            tok_copy(a, 2, q, tok_block(a, core, q), across).start()
        relay(a, q).start()

    def relayed(a):
        for q in (at_near, at_across, at_both):
            remote(tok_block(a, 1 - core, q), tok_block(a, 1 - core, q), relay_send.at[a, q], relay_recv.at[a, q], sibling).wait_recv()

    def project(h, kind, groups, first=False):
        a, w, count, into = ((0, 0, 2, back_acc), (2, 2, 1, down_acc), (1, 0, 2, fwd_acc))[kind]
        wide = count * pads[h]
        at_rows = both_rows(w, h, count)
        for t in range(2):
            at_tokens = pl.ds(t * slab, slab)
            value = None if first else into[h, at_tokens, :wide]
            for s, line in groups:
                at = pl.ds(pl.multiple_of((s * 4 + line * 2) * depth, 2 * depth), 2 * depth)
                term = wide_dot(toks[a, at_tokens, at], weights[at_rows, at])
                value = term if value is None else value + term
            into[h, at_tokens, :wide] = value

    piece = 64

    def back_parts(h):
        n = pads[h]

        @pl.loop(0, 2 * slab // piece)
        def _(r):
            at = pl.ds(pl.multiple_of(r * piece, piece), piece)
            gate, up = back_acc[h, at, :n], back_acc[h, at, n : 2 * n]
            s = jax.nn.sigmoid(gate)
            back = 0.5 * down_acc[h, at, :n]
            gate_diff = (back * up * s * (1.0 + gate * (1.0 - s))).astype(jnp.bfloat16)
            diff_cols[h, at, :n] = gate_diff
            diffs[h, at, :n] = gate_diff
            diffs[h, at, n : 2 * n] = (back * gate * s).astype(jnp.bfloat16)

    def fwd_parts(h):
        n = pads[h]

        @pl.loop(0, 2 * slab // piece)
        def _(r):
            at = pl.ds(pl.multiple_of(r * piece, piece), piece)
            gate, up = fwd_acc[h, at, :n], fwd_acc[h, at, n : 2 * n]
            hidden[h, at, :n] = (gate * jax.nn.sigmoid(gate) * up).astype(jnp.bfloat16)

    def grad_rows(h):
        return pl.ds(starts[h], sizes[h])

    def grad_across(h, n):
        pair = pl.ds((other, far, near, z)[n] * 2, 2)
        return remote(
            grad_send.at[1 - x, pair, grad_rows(h)], grad_side.at[pair, grad_rows(h)], gside_send.at[h, n], gside_recv.at[h, n], beside
        )

    def grad_make(h):
        diff_turned = diff_cols[h, :, : sizes[h]].T
        for s in range(4):
            at = level_lanes(s)
            product = jnp.dot(diff_turned, toks[0, :, at], preferred_element_type=jnp.float32)
            product = product.astype(jnp.bfloat16)
            for q in range(4):
                grad_send[q % 2, s * 2 + q // 2, grad_rows(h), :] = product[:, q * depth : (q + 1) * depth]

    def grad_out(h):
        for s in range(4):
            grad_across(h, s).start()

    def grad_to(h, n):
        s = (near, far, other)[n]
        source = grad_total.at[pl.ds(s * 2, 2), grad_rows(h)]
        return remote(source, grad_recv.at[n, :, grad_rows(h)], glev_send.at[h, n], glev_recv.at[h, n], chip(x, y, s))

    def grad_past(h):
        source = grad_total.at[pl.ds(other * 2, 2), grad_rows(h)]
        return remote(source, grad_pass.at[:, grad_rows(h)], gpass_send.at[h], gpass_recv.at[h], chip(x, y, far))

    def grad_turned(h):
        return remote(
            grad_turn.at[:, grad_rows(h)], turn_recv.at[:, grad_rows(h)], gturn_send.at[h], gturn_recv.at[h], across
        )

    def grad_on(h, n):
        grad_across(h, n).wait_recv()
        for line in range(2):
            j = (other, far, near, z)[n] * 2 + line
            total = grad_send[x, j, grad_rows(h), :].astype(jnp.float32) + grad_side[j, grad_rows(h), :].astype(jnp.float32)
            grad_total[j, grad_rows(h), :] = total.astype(jnp.bfloat16)
        if n == 0:

            @pl.when(inner)
            def _():
                grad_to(h, 2).start()

            @pl.when(jnp.logical_not(inner))
            def _():
                grad_past(h).start()

        if n == 1:
            grad_to(h, 1).start()
        if n == 2:

            @pl.when(jnp.logical_not(inner))
            def _():
                grad_to(h, 0).start()

    def grad_mid(h):
        @pl.when(inner)
        def _():
            grad_past(h).wait_recv()
            for line in range(2):
                j = near * 2 + line
                total = grad_total[j, grad_rows(h), :].astype(jnp.float32) + grad_pass[line, grad_rows(h), :].astype(jnp.float32)
                grad_total[j, grad_rows(h), :] = total.astype(jnp.bfloat16)
            grad_to(h, 0).start()

    def grad_cols_at(h, to_y, to_odd):
        return pl.ds(pl.multiple_of((to_y * 2 + to_odd) * rows + starts[h], 16), sizes[h])

    def grad_cross(h):
        at = grad_rows(h)
        for n in range(2):
            grad_to(h, n).wait_recv()

        @pl.when(inner)
        def _():
            grad_to(h, 2).wait_recv()
            for line in range(2):
                total = grad_recv[0, line, at, :].astype(jnp.float32) + grad_recv[2, line, at, :].astype(jnp.float32)
                grad_recv[0, line, at, :] = total.astype(jnp.bfloat16)

        def sums(line):
            same = grad_total[z * 2 + line, at, :].astype(jnp.float32) + grad_recv[1, line, at, :].astype(jnp.float32)
            return same, grad_recv[0, line, at, :]

        same, unlike = sums(1 - y)
        grad_turn[0, at, :] = same.astype(jnp.bfloat16)
        grad_turn[1, at, :] = unlike
        grad_turned(h).start()
        same, unlike = sums(y)
        grad_cols[grad_cols_at(h, y, odd), :] = same
        grad_cols[grad_cols_at(h, y, 1 - odd), :] = unlike.astype(jnp.float32)

    def grad_in(h):
        grad_turned(h).wait_recv()
        for n, to_odd in enumerate((odd, 1 - odd)):
            grad_cols[grad_cols_at(h, 1 - y, to_odd), :] = turn_recv[n, grad_rows(h), :].astype(jnp.float32)

    span = width // 2

    def columns(c):
        return pl.ds(c * span, span)

    def cross(k, c):
        at = columns(c)
        return remote(
            part.at[k, 1 - core, :, at], crossed.at[k, :, at], cross_sem.at[k, c, 0], cross_sem.at[k, c, 1], sibling
        )

    strip = 512

    def product_of(k, h, rows_at, at):
        n = pads[h]
        if k == 0:
            return jnp.dot(hidden[h, rows_at, :n], weights[both_rows(2, h), at], preferred_element_type=jnp.float32)
        return jnp.dot(diffs[h, rows_at, : 2 * n], weights[both_rows(0, h, 2), at], preferred_element_type=jnp.float32)

    def partial(k, t, c):
        rows_at = pl.ds(pl.multiple_of(t * slab, slab), slab)
        at = columns(c)
        part[k, t, :, at] = (product_of(k, 0, rows_at, at) + product_of(k, 1, rows_at, at)).astype(jnp.bfloat16)

    routes = ((across, at_across, at_near, chip(x, y, near)), (chip(x, y, near), at_near, at_across, across))
    routed = ((0, 0), (1, 0))
    def join_copy(k, c, n):
        to, theirs, mine, on = routes[routed[k][c]]
        at = columns(c)
        if n == 2:
            source, device = folded.at[k, :, at], on
        else:
            source, device = joined.at[k, (at_both, theirs)[n], :, at], to
        return remote(source, gathered.at[k, n, :, at], join_send.at[k, c, n], join_recv.at[k, c, n], device)

    def join_start(k, c):
        cross(k, c).wait_recv()
        at = columns(c)
        for n, q in enumerate((at_both, *routes[routed[k][c]][1:3], me)):
            rows_at = pl.ds(pl.multiple_of(q * half, half), half)
            total = part[k, core, rows_at, at].astype(jnp.float32) + crossed[k, rows_at, at].astype(jnp.float32)
            joined[k, q, :, at] = total.astype(jnp.bfloat16)
            if n < 2:
                join_copy(k, c, n).start()

    def join_fold(k, c):
        at = columns(c)
        join_copy(k, c, 0).wait_recv()
        total = gathered[k, 0, :, at].astype(jnp.float32) + joined[k, routes[routed[k][c]][2], :, at].astype(jnp.float32)
        folded[k, :, at] = total.astype(jnp.bfloat16)
        join_copy(k, c, 2).start()

    def stages_in(h):
        for w in range(3):
            stage_in(w, h)

    first_far = (jnp.where(inner, other, far), jnp.where(inner, y, y_flip))
    next_far = (other, jnp.where(inner, y_flip, y))
    last_far = (jnp.where(inner, far, other), y_flip)
    home = ((z, y), (z, y_flip))
    soon = ((near, y), (far, y), first_far)
    late = ((near, y_flip), next_far, last_far)

    def down_parts(k):
        for c in range(2):
            partial(k, 1 - core, c)
            cross(k, c).start()
        for c in range(2):
            partial(k, core, c)

    for w in range(3):
        turn_in(w)
        if w == 0:
            pl.semaphore_wait(barrier, 9)
        send_stage(0, (w,))
        send_own(0, (w,))
    token_copies[2].wait()
    send_tokens(2, 1)
    send_tokens(2, 0)
    token_copies[0].wait()
    normal(0)
    send_tokens(0, 1)
    send_tokens(0, 0)
    send_own(1)
    token_copies[1].wait()
    normal(1)
    clear_pads()
    for h in range(2):
        keep_own(h)
    for a in range(3):
        keep_tokens(a)
    stages_in(0)
    send_tokens(1, 0)
    line_in(0, near, y)
    line_in(0, far, y)
    tok_in(2, at_across)
    tok_in(2, at_near)
    send_stage(1)
    line_in(0, *first_far)
    tok_in(0, at_across)
    line_in(1, far, y)
    tok_in(0, at_near)
    send_tokens(1, 1)
    line_in(0, *next_far)
    line_in(1, near, y)
    stages_in(1)
    tok_in(2, at_both)
    line_in(0, near, y_flip)
    relayed(2)
    line_in(1, *first_far)
    sides_in(0, home)
    project(0, 1, home, True)
    tok_in(0, at_both)
    line_in(1, *next_far)
    relayed(0)
    project(0, 0, home, True)
    tok_in(1, at_across)
    sides_in(0, soon)
    project(0, 1, soon)
    line_in(0, *last_far)
    project(0, 0, soon)
    tok_in(1, at_near)
    sides_in(1, home)
    project(1, 0, home, True)
    project(1, 1, home, True)
    line_in(1, near, y_flip)
    line_in(1, *last_far)
    sides_in(1, soon)
    project(1, 0, soon)
    project(1, 1, soon)
    sides_in(0, late)
    project(0, 1, late)
    project(0, 0, late)
    back_parts(0)
    grad_make(0)
    grad_out(0)
    tok_in(1, at_both)
    sides_in(1, late)
    project(1, 0, late)
    project(1, 1, late)
    back_parts(1)
    down_parts(1)
    grad_make(1)
    grad_out(1)
    for c in range(2):
        join_start(1, c)
    relayed(1)
    project(0, 2, home + soon + late, True)
    fwd_parts(0)
    grad_on(0, 0)
    project(1, 2, home + soon + late, True)
    fwd_parts(1)
    down_parts(0)
    grad_on(0, 1)
    for c in range(2):
        join_start(0, c)
    grad_on(0, 2)
    grad_on(0, 3)
    grad_mid(0)
    for c in range(2):
        join_fold(1, c)
    for n in range(4):
        grad_on(1, n)
    grad_mid(1)
    for c in range(2):
        join_fold(0, c)
    grad_cross(0)
    grad_cross(1)

    mine = pl.ds(pl.multiple_of(core * half, half), half)

    def last(k):
        out = (fwd_out, back_out)[k].at[mine, :]
        return remote(out, out, last_sem.at[k, 0], last_sem.at[k, 1], sibling)

    def joined_in(k):
        for c in range(2):
            for n in (1, 2):
                join_copy(k, c, n).wait_recv()

    def total_of(k, at):
        value = joined[k, me, at, :].astype(jnp.float32) + gathered[k, 1, at, :].astype(jnp.float32)
        return value + gathered[k, 2, at, :].astype(jnp.float32)

    tiles = grad_cols.shape[0] // 128
    early = rows * 2 // 128

    def grad_tiles(first, count):
        @pl.loop(0, count)
        def _(n):
            at = pl.ds(pl.multiple_of((first + n) * 128, 128), 128)
            sum_out[:, at] = sum_ref[:, at] + grad_cols[at, :].T

    small = 16

    def out_rows(r):
        return pl.ds(pl.multiple_of(core * half + r * small, small), small)

    sum_copy.wait()
    grad_tiles(y * (tiles - early), early)
    joined_in(0)
    for r in range(half // small):
        fwd_out[out_rows(r), :] = (0.5 * total_of(0, pl.ds(r * small, small))).astype(jnp.bfloat16)
    last(0).start()
    joined_in(1)
    for r in range(half // small):
        values = tokens_ref[out_rows(r), :].astype(jnp.float32)
        factor = lax.rsqrt(jnp.mean(values * values, axis=-1, keepdims=True) + norm_eps)
        scaled = total_of(1, pl.ds(r * small, small)) * gain_ref[...]
        cubed = factor * factor * factor
        back_out[out_rows(r), :] = (
            factor * scaled - values * cubed * jnp.mean(scaled * values, axis=-1, keepdims=True)
        ).astype(jnp.bfloat16)
    last(1).start()

    for h in range(2):
        grad_in(h)
    grad_tiles((1 - y) * early, tiles - early)

    for h in range(2):
        for w in range(3):
            for n in range(2):
                gone = block(w, h, fs)
                for sem in (stage_send, near_send, far_send):
                    send_block(w, h, fs, gone, sem.at[w, h, n], sibling).wait_send()

                @pl.when(inner)
                def _():
                    for sem in (other_send, pass_send):
                        send_block(w, h, fs, gone, sem.at[w, h, n], sibling).wait_send()

            @pl.loop(0, 8)
            def _(j):
                send_block(w, h, fs, gone, side_send.at[w, h, j], sibling).wait_send()

        for s in range(4):
            grad_across(h, s).wait_send()
        grad_to(h, 0).wait_send()
        grad_to(h, 1).wait_send()
        grad_turned(h).wait_send()

        @pl.when(inner)
        def _():
            grad_to(h, 2).wait_send()

        @pl.when(jnp.logical_not(inner))
        def _():
            grad_past(h).wait_send()

    for a in range(3):
        for n in range(3):
            tok_copy(a, n, me, tok_block(a, core, me), sibling).wait_send()
        for q in (at_near, at_across, at_both):
            relay(a, q).wait_send()
    for k in range(2):
        for c in range(2):
            cross(k, c).wait_send()
            for n in range(3):
                join_copy(k, c, n).wait_send()
        last(k).wait()


def fused_shards(
    split, fwd_tokens, back_tokens, out_grad, norm_gain, gate_weight, up_weight, down_weight, gate_grad_sum
):
    tokens, width = fwd_tokens.shape
    depth, cols = gate_weight.shape
    rows = cols // 4
    out_bytes = 2 * tokens * width * 2 + depth * cols * 4
    wide = max(padded(split), padded(rows - split))
    held = 3 * (padded(split) + padded(rows - split))
    half = tokens // 2
    slab = half * 4
    narrow, full = jnp.bfloat16, jnp.float32
    dma = pltpu.SemaphoreType.DMA
    vmem = pl.BlockSpec(memory_space=pltpu.VMEM)
    hbm = pl.BlockSpec(memory_space=pl.ANY)
    return pl.pallas_call(
        functools.partial(layer_kernel, split),
        out_shape=(
            pltpu.VMEM((tokens, width), narrow),
            pltpu.VMEM((tokens, width), narrow),
            pltpu.VMEM((depth, cols), full),
        ),
        in_specs=[hbm] * 3 + [vmem] + [hbm] * 4,
        out_specs=(vmem,) * 3,
        scratch_shapes=[
            pltpu.VMEM((3, depth, cols), narrow),
            pltpu.VMEM((3, tokens, width), narrow),
            pltpu.VMEM((depth, cols), full),
            pltpu.VMEM((3, cols, depth), narrow),
            pltpu.VMEM((2, tokens, width), narrow),
            pltpu.VMEM((3, 2 * slab, width), narrow),
            pltpu.VMEM((held, width), narrow),
            pltpu.VMEM((held, depth), narrow),
            pltpu.VMEM((2, 2 * slab, 2 * wide), full),
            pltpu.VMEM((2, 2 * slab, wide), full),
            pltpu.VMEM((2, 2 * slab, 2 * wide), full),
            pltpu.VMEM((2, 2 * slab, wide), narrow),
            pltpu.VMEM((2, 2 * slab, 2 * wide), narrow),
            pltpu.VMEM((2, 2 * slab, wide), narrow),
            pltpu.VMEM((2, 2, slab, width), narrow),
            pltpu.VMEM((2, slab, width), narrow),
            pltpu.VMEM((2, 4, half, width), narrow),
            pltpu.VMEM((2, half, width), narrow),
            pltpu.VMEM((2, 3, half, width), narrow),
            pltpu.VMEM((2, 8, rows, depth), narrow),
            pltpu.VMEM((8, rows, depth), narrow),
            pltpu.VMEM((8, rows, depth), narrow),
            pltpu.VMEM((2, rows, depth), narrow),
            pltpu.VMEM((3, 2, rows, depth), narrow),
            pltpu.VMEM((2, rows, depth), narrow),
            pltpu.VMEM((2, rows, depth), narrow),
            pltpu.VMEM((cols, depth), full),
            dma((3, 2, 2)),
            dma((3, 2)),
            dma((3, 2, 16)),
            dma((3, 2, 2)),
            dma((3, 2, 2)),
            dma((3, 2, 2)),
            dma((3, 2, 2)),
            dma((3, 2, 8)),
            dma((3, 3)),
            dma((3, 4)),
            dma((3, 4)),
            dma((3, 4)),
            dma((2, 4)),
            dma((2, 4)),
            dma((2, 3)),
            dma((2, 3)),
            dma((2,)),
            dma((2,)),
            dma((2,)),
            dma((2,)),
            dma((2, 2, 2)),
            dma((2, 2, 3)),
            dma((2, 2, 3)),
            dma((2, 2)),
            dma((3,)),
            dma((3,)),
            dma((1,)),
        ],
        compiler_params=pltpu.CompilerParams(
            collective_id=0, has_side_effects=True, vmem_limit_bytes=vmem_bytes - out_bytes
        ),
    )(
        fwd_tokens, back_tokens, out_grad, norm_gain.reshape(1, width),
        gate_weight, up_weight, down_weight, gate_grad_sum,
    )


def body_for(mesh):
    def body(*args):
        tokens, width = args[0].shape
        depth, cols = args[4].shape
        rows = cols // 4
        fits = (
            mesh.shape["tp"] == 2 and mesh.shape["fs"] == 16
            and depth == 128 and width == 16 * depth and cols % 128 == 0 and tokens % 128 == 0
            and rows > 256 and rows % 16 == 0
        )
        if not fits:
            return shards(*args)
        return fused_shards((rows - 1) // 256 * 256, *args)

    return body


def solution(mesh):
    in_specs = (
        P("fs", None),
        P("fs", None),
        P("fs", None),
        P(),
        P("fs", "tp"),
        P("fs", "tp"),
        P("fs", "tp"),
        P("fs", "tp"),
    )
    out_specs = (P("fs", None), P("fs", None), P("fs", "tp"))
    return jax.shard_map(body_for(mesh), mesh=mesh, in_specs=in_specs, out_specs=out_specs, check_vma=False)
```

```python
import functools

import jax
import jax.numpy as jnp
from jax import lax
from jax.experimental import pallas as pl
from jax.experimental.pallas import tpu as pltpu
from jax.sharding import PartitionSpec as P

norm_eps = 0.25
vmem_bytes = 66_900_000


def normalize(tokens, norm_gain):
    values = tokens.astype(jnp.float32)
    factor = lax.rsqrt(jnp.mean(values * values, axis=-1, keepdims=True) + norm_eps)
    return (values, factor, (values * factor * norm_gain).astype(jnp.bfloat16))


def shards(
    fwd_tokens, back_tokens, out_grad, norm_gain, gate_weight, up_weight, down_weight, gate_grad_sum
):
    fwd_normed = normalize(fwd_tokens, norm_gain)[2]
    columns = fwd_normed
    gate_pre = jnp.dot(
        columns,
        lax.all_gather(gate_weight, "fs", axis=0, tiled=True),
        preferred_element_type=jnp.float32,
    )
    up_pre = jnp.dot(
        columns,
        lax.all_gather(up_weight, "fs", axis=0, tiled=True),
        preferred_element_type=jnp.float32,
    )
    hidden = (gate_pre * jax.nn.sigmoid(gate_pre) * up_pre).astype(jnp.bfloat16)
    partial_value = jnp.dot(
        hidden,
        lax.all_gather(down_weight, "fs", axis=0, tiled=True).T,
        preferred_element_type=jnp.float32,
    )
    summed = lax.psum(partial_value.astype(jnp.bfloat16), "tp").astype(jnp.float32)
    fwd_out = (0.5 * summed).astype(jnp.bfloat16)
    gate_whole = lax.all_gather(gate_weight, "fs", axis=0, tiled=True)
    up_whole = lax.all_gather(up_weight, "fs", axis=0, tiled=True)
    down_whole = lax.all_gather(down_weight, "fs", axis=0, tiled=True)
    values, factor, back_normed = normalize(back_tokens, norm_gain)
    gate_pre = jnp.dot(back_normed, gate_whole, preferred_element_type=jnp.float32)
    up_pre = jnp.dot(back_normed, up_whole, preferred_element_type=jnp.float32)
    sigmoid_gate = jax.nn.sigmoid(gate_pre)
    back_hidden = 0.5 * jnp.dot(out_grad, down_whole, preferred_element_type=jnp.float32)
    gate_diff = (
        back_hidden * up_pre * sigmoid_gate * (1.0 + gate_pre * (1.0 - sigmoid_gate))
    ).astype(jnp.bfloat16)
    up_diff = (back_hidden * gate_pre * sigmoid_gate).astype(jnp.bfloat16)
    columns = back_normed
    gate_grad_out = gate_grad_sum + lax.psum_scatter(
        jnp.dot(columns.T, gate_diff, preferred_element_type=jnp.float32),
        "fs",
        scatter_dimension=0,
        tiled=True,
    )
    partial_diff = jnp.dot(gate_diff, gate_whole.T, preferred_element_type=jnp.float32)
    partial_diff = partial_diff + jnp.dot(up_diff, up_whole.T, preferred_element_type=jnp.float32)
    normed_diff = lax.psum(partial_diff.astype(jnp.bfloat16), "tp").astype(jnp.float32)
    scaled = normed_diff * norm_gain
    cubed = factor * factor * factor
    back_grad = (
        factor * scaled - values * cubed * jnp.mean(scaled * values, axis=-1, keepdims=True)
    ).astype(jnp.bfloat16)
    back_grad, gate_grad_out = (back_grad, gate_grad_out)
    return (fwd_out, back_grad, gate_grad_out)


MESH = pl.DeviceIdType.MESH


def wide_dot(a, b):
    return lax.dot_general(a, b, (((1,), (1,)), ((), ())), preferred_element_type=jnp.float32)


def padded(size):
    return (size + 127) // 128 * 128


def layer_kernel(
    split, fwd_in, tokens_in, grad_in_ref, gain_ref, gate_in, up_in, down_in, sum_in,
    fwd_out, back_out, sum_out,
    raw, raw_tokens, sum_ref, turned, normed, toks, weights, staged, back_acc, down_acc, fwd_acc, hidden, diffs, diff_cols,
    part, crossed, joined, folded, gathered, grad_send, grad_side, grad_total, grad_pass, grad_recv, grad_turn, turn_recv, grad_cols,
    block_send, inner_send, line_recv, held_recv, side_recv, tok_send, tok_recv, relay_recv,
    gside_send, gside_recv, gsend, glev_recv, gpass_recv, gturn_recv,
    cross_send, cross_recv, join_send, fold_recv, join_recv, last_send, last_recv, raw_sem, token_sem, sum_sem,
):
    fs, core = lax.axis_index("fs"), lax.axis_index("tp")
    x, y, z = fs % 2, fs // 2 % 2, fs // 4
    odd = z % 2
    inner = jnp.logical_and(z > 0, z < 3)
    near, far, other = z + 1 - 2 * odd, (z + 2) % 4, 3 - z
    sibling = (fs, 1 - core)
    rows = turned.shape[1] // 4
    starts, sizes = (0, split), (split, rows - split)
    pads = tuple(padded(size) for size in sizes)
    depth = gate_in.shape[0]
    half = fwd_in.shape[0] // 2
    tokens_ref, fwd_ref, grad_ref = raw_tokens.at[0], raw_tokens.at[1], raw_tokens.at[2]
    slab = half * 4
    width = fwd_in.shape[1]
    band = 4 * depth

    def chip(to_x, to_y, to_z):
        return (to_z * 4 + to_y * 2 + to_x, core)

    beside, across = chip(1 - x, y, z), chip(x, 1 - y, z)
    y_flip = 1 - y

    barrier = pltpu.get_barrier_semaphore()
    for device in (
        sibling, beside, across, chip(x, y, near), chip(x, y, far), chip(x, y, other),
        chip(x, 1 - y, near), chip(x, 1 - y, far), chip(x, 1 - y, other),
    ):
        pl.semaphore_signal(barrier, inc=1, device_id=device, device_id_type=MESH)

    raw_copies = [pltpu.make_async_copy(ref, raw.at[w], raw_sem.at[w]) for w, ref in enumerate((gate_in, up_in, down_in))]
    token_copies = [
        pltpu.make_async_copy(ref, raw_tokens.at[a], token_sem.at[a]) for a, ref in enumerate((tokens_in, fwd_in, grad_in_ref))
    ]
    sum_copy = pltpu.make_async_copy(sum_in, sum_ref, sum_sem.at[0])
    for copy in (*raw_copies, token_copies[2], token_copies[0], token_copies[1], sum_copy):
        copy.start()

    def turn_in(w):
        raw_copies[w].wait()
        for n in range(turned.shape[1] // 128):
            at = pl.ds(n * 128, 128)
            turned[w, at, :] = raw[w, :, at].T

    def remote(src, dst, send, recv, device):
        return pltpu.make_async_remote_copy(
            src_ref=src, dst_ref=dst, send_sem=send, recv_sem=recv, device_id=device, device_id_type=MESH
        )

    def got(ref, sem):
        remote(ref, ref, sem, sem, sibling).wait_recv()

    def gone(ref, sem):
        remote(ref, ref, sem, sem, sibling).wait_send()

    def own_rows(h, to_y, to_odd):
        return pl.ds(pl.multiple_of((to_y * 2 + to_odd) * rows + starts[h], 16), sizes[h])

    def held_rows(w, h):
        return pl.ds(3 * starts[h] + w * pads[h], sizes[h])

    def both_rows(w, h, count=1):
        return pl.ds(3 * starts[h] + w * pads[h], count * pads[h])

    def own(w, h, to_y, to_odd):
        return turned.at[w, own_rows(h, to_y, to_odd), :]

    def lanes(src):
        return pl.ds(pl.multiple_of(src * depth, depth), depth)

    def level_lanes(s):
        return pl.ds(pl.multiple_of(s * band, band), band)

    def block(w, h, src):
        return weights.at[held_rows(w, h), lanes(src)]

    def send_block(w, h, src, source, device, recv, send):
        return remote(source, block(w, h, src), send.at[0], recv, device)

    def line_sem(w, h, role):
        return line_recv.at[w if h == 0 else 3, role]

    def held_sem(w, h):
        return held_recv.at[w if h == 0 else 3]

    def block_in(w, h, sem):
        if h == 0:
            got(weights.at[pl.ds(0, sizes[0]), pl.ds(0, depth)], sem)
        elif w == 0:
            got(weights.at[pl.ds(0, 3 * sizes[1]), pl.ds(0, depth)], sem)

    def to_near(w, h, src, source, line):
        send_block(w, h, src, source, chip(x, y, near), line_sem(w, h, 1 + line), block_send).start()

    def to_far(w, h, src, source, line):
        send_block(w, h, src, source, chip(x, y, far), line_sem(w, h, 3 + line), block_send).start()

    def to_other(w, h, src, source, line):
        @pl.when(inner)
        def _():
            send_block(w, h, src, source, chip(x, y, other), line_sem(w, h, 5 + line), inner_send).start()

    def pass_far(w, h, src, source, line):
        @pl.when(inner)
        def _():
            send_block(w, h, src, source, chip(x, y, far), line_sem(w, h, 5 + line), inner_send).start()

    def side(w, h, src, source, bundle):
        send_block(w, h, src, source, beside, side_recv.at[h, bundle], block_send).start()

    def send_stage(h, some=range(3)):
        for w in some:
            send_block(w, h, fs, own(w, h, 1 - y, odd), across, line_sem(w, h, 0), block_send).start()
            remote(
                own(w, h, 1 - y, 1 - odd), staged.at[held_rows(w, h), :], block_send.at[0], held_sem(w, h), across
            ).start()

    def send_own(h, some=range(3)):
        for w in some:
            to_near(w, h, fs, own(w, h, y, 1 - odd), 0)
            to_far(w, h, fs, own(w, h, y, odd), 0)
            side(w, h, fs, own(w, h, y, odd), 0)

    def send_others(h):
        for w in range(3):
            to_other(w, h, fs, own(w, h, y, 1 - odd), 0)
        for w in range(3):
            to_other(w, h, z * 4 + (1 - y) * 2 + x, staged.at[held_rows(w, h), :], 1)

    def keep_own(h):
        for w in range(3):
            weights[held_rows(w, h), lanes(fs)] = turned[w, own_rows(h, y, odd), :]

    def clear_pads():
        for h in range(2):
            if pads[h] > sizes[h]:
                for w in range(3):
                    gap = pl.ds(3 * starts[h] + w * pads[h] + sizes[h], pads[h] - sizes[h])
                    weights[gap, :] = jnp.zeros((pads[h] - sizes[h], width), jnp.bfloat16)

    def stage_in(w, h):
        src = z * 4 + (1 - y) * 2 + x
        held = staged.at[held_rows(w, h), :]
        block_in(w, h, held_sem(w, h))
        to_near(w, h, src, held, 1)
        block_in(w, h, line_sem(w, h, 0))
        to_far(w, h, src, block(w, h, src), 1)
        side(w, h, src, block(w, h, src), 0)

    def line_in(h, group, passed=None):
        s, line, role, bundle = group
        for w in range(3):
            src = s * 4 + line * 2 + x
            block_in(w, h, line_sem(w, h, role))
            if passed is not None:
                pass_far(w, h, src, block(w, h, src), passed)
            side(w, h, src, block(w, h, src), bundle)

    def sides_in(h, groups):
        got(weights.at[pl.ds(0, 3 * sizes[h]), pl.ds(0, len(groups) * depth)], side_recv.at[h, groups[0][3]])

    me = y * 2 + odd
    at_near, at_across, at_both = y * 2 + 1 - odd, (1 - y) * 2 + odd, (1 - y) * 2 + 1 - odd

    def token_rows(a, at):
        return grad_ref.at[at, :] if a == 2 else normed.at[a, at, :]

    def tok_block(a, h, q, n=None):
        rows_of = half if n is None else half // 2
        first = h * slab + q * half + (0 if n is None else n * rows_of)
        return toks.at[a, pl.ds(pl.multiple_of(first, rows_of), rows_of), :]

    def tok_copy(a, q, source, device, role, n=None):
        return remote(source, tok_block(a, core, q, n), tok_send.at[0], tok_recv.at[a, role], device)

    def relay(a, q, n=None):
        block_of = tok_block(a, core, q, n)
        return remote(block_of, block_of, tok_send.at[0], relay_recv.at[a], sibling)

    def tok_pieces(a):
        return (None,) if a != 1 else (0, 1)

    def send_tokens(a, role):
        for n in tok_pieces(a) if role == 0 else (None,):
            rows_of = half if n is None else half // 2
            mine = token_rows(a, pl.ds(pl.multiple_of(core * half + (n or 0) * rows_of, rows_of), rows_of))
            tok_copy(a, me, mine, (chip(x, y, near), across)[role], role + 3 * (n or 0), n).start()

    def normal(a):
        @pl.loop(0, tokens_ref.shape[0] // 16)
        def _(r):
            at = pl.ds(pl.multiple_of(r * 16, 16), 16)
            normed[a, at, :] = normalize((tokens_ref, fwd_ref)[a][at, :], gain_ref[...])[2]

    def keep_tokens(a):
        for h in range(2):
            toks[a, pl.ds(pl.multiple_of(h * slab + me * half, half), half), :] = token_rows(a, pl.ds(h * half, half))[...]

    def tok_in(a, q):
        role = [q is at for at in (at_near, at_across, at_both)].index(True)
        for n in tok_pieces(a) if role != 1 else (None,):
            got(tok_block(a, core, q, n), tok_recv.at[a, role + 3 * (n or 0)])
            if role == 0:
                tok_copy(a, q, tok_block(a, core, q, n), across, 2 + 3 * (n or 0), n).start()
            relay(a, q, n).start()

    def relayed(a):
        got(toks.at[a, pl.ds(0, 3 * half), :], relay_recv.at[a])

    def project(h, kind, groups, first=False):
        a, w, count, into = ((0, 0, 2, back_acc), (2, 2, 1, down_acc), (1, 0, 2, fwd_acc))[kind]
        wide = count * pads[h]
        at_rows = both_rows(w, h, count)
        for t in range(2):
            at_tokens = pl.ds(t * slab, slab)
            value = None if first else into[h, at_tokens, :wide]
            for s, line, _, _ in groups:
                at = pl.ds(pl.multiple_of((s * 4 + line * 2) * depth, 2 * depth), 2 * depth)
                term = wide_dot(toks[a, at_tokens, at], weights[at_rows, at])
                value = term if value is None else value + term
            into[h, at_tokens, :wide] = value

    piece = 64

    def back_parts(h):
        n = pads[h]

        @pl.loop(0, 2 * slab // piece)
        def _(r):
            at = pl.ds(pl.multiple_of(r * piece, piece), piece)
            gate, up = back_acc[h, at, :n], back_acc[h, at, n : 2 * n]
            s = jax.nn.sigmoid(gate)
            back = 0.5 * down_acc[h, at, :n]
            gate_diff = (back * up * s * (1.0 + gate * (1.0 - s))).astype(jnp.bfloat16)
            diff_cols[h, at, :n] = gate_diff
            diffs[h, at, :n] = gate_diff
            diffs[h, at, n : 2 * n] = (back * gate * s).astype(jnp.bfloat16)

    def fwd_parts(h):
        n = pads[h]

        @pl.loop(0, 2 * slab // piece)
        def _(r):
            at = pl.ds(pl.multiple_of(r * piece, piece), piece)
            gate, up = fwd_acc[h, at, :n], fwd_acc[h, at, n : 2 * n]
            hidden[h, at, :n] = (gate * jax.nn.sigmoid(gate) * up).astype(jnp.bfloat16)

    def grad_rows(h):
        return pl.ds(starts[h], sizes[h])

    def grad_across(h, n):
        pair = pl.ds((other, far, near, z)[n] * 2, 2)
        return remote(
            grad_send.at[1 - x, pair, grad_rows(h)], grad_side.at[pair, grad_rows(h)], gside_send.at[0], gside_recv.at[h, n], beside
        )

    def grad_make(h):
        diff_turned = diff_cols[h, :, : sizes[h]].T
        for s in range(4):
            at = level_lanes(s)
            product = jnp.dot(diff_turned, toks[0, :, at], preferred_element_type=jnp.float32)
            product = product.astype(jnp.bfloat16)
            for q in range(4):
                grad_send[q % 2, s * 2 + q // 2, grad_rows(h), :] = product[:, q * depth : (q + 1) * depth]

    def grad_out(h):
        for s in range(4):
            grad_across(h, s).start()

    def grad_to(h, n):
        s = (near, far, other)[n]
        source = grad_total.at[pl.ds(s * 2, 2), grad_rows(h)]
        return remote(source, grad_recv.at[n, :, grad_rows(h)], gsend.at[0], glev_recv.at[h, n], chip(x, y, s))

    def grad_past(h):
        source = grad_total.at[pl.ds(other * 2, 2), grad_rows(h)]
        return remote(source, grad_pass.at[:, grad_rows(h)], gsend.at[0], gpass_recv.at[h], chip(x, y, far))

    def grad_turned(h):
        return remote(
            grad_turn.at[:, grad_rows(h)], turn_recv.at[:, grad_rows(h)], gsend.at[0], gturn_recv.at[h], across
        )

    def grad_on(h, n):
        grad_across(h, n).wait_recv()
        for line in range(2):
            j = (other, far, near, z)[n] * 2 + line
            total = grad_send[x, j, grad_rows(h), :].astype(jnp.float32) + grad_side[j, grad_rows(h), :].astype(jnp.float32)
            grad_total[j, grad_rows(h), :] = total.astype(jnp.bfloat16)
        if n == 0:

            @pl.when(inner)
            def _():
                grad_to(h, 2).start()

            @pl.when(jnp.logical_not(inner))
            def _():
                grad_past(h).start()

        if n == 1:
            grad_to(h, 1).start()
        if n == 2:

            @pl.when(jnp.logical_not(inner))
            def _():
                grad_to(h, 0).start()

    def grad_mid(h):
        @pl.when(inner)
        def _():
            grad_past(h).wait_recv()
            for line in range(2):
                j = near * 2 + line
                total = grad_total[j, grad_rows(h), :].astype(jnp.float32) + grad_pass[line, grad_rows(h), :].astype(jnp.float32)
                grad_total[j, grad_rows(h), :] = total.astype(jnp.bfloat16)
            grad_to(h, 0).start()

    def grad_cols_at(h, to_y, to_odd):
        return pl.ds(pl.multiple_of((to_y * 2 + to_odd) * rows + starts[h], 16), sizes[h])

    def grad_cross(h):
        at = grad_rows(h)
        for n in range(2):
            grad_to(h, n).wait_recv()

        @pl.when(inner)
        def _():
            grad_to(h, 2).wait_recv()
            for line in range(2):
                total = grad_recv[0, line, at, :].astype(jnp.float32) + grad_recv[2, line, at, :].astype(jnp.float32)
                grad_recv[0, line, at, :] = total.astype(jnp.bfloat16)

        def sums(line):
            same = grad_total[z * 2 + line, at, :].astype(jnp.float32) + grad_recv[1, line, at, :].astype(jnp.float32)
            return same, grad_recv[0, line, at, :]

        same, unlike = sums(1 - y)
        grad_turn[0, at, :] = same.astype(jnp.bfloat16)
        grad_turn[1, at, :] = unlike
        grad_turned(h).start()
        same, unlike = sums(y)
        grad_cols[grad_cols_at(h, y, odd), :] = same
        grad_cols[grad_cols_at(h, y, 1 - odd), :] = unlike.astype(jnp.float32)

    def grad_in(h):
        grad_turned(h).wait_recv()
        for n, to_odd in enumerate((odd, 1 - odd)):
            grad_cols[grad_cols_at(h, 1 - y, to_odd), :] = turn_recv[n, grad_rows(h), :].astype(jnp.float32)

    span = width // 2

    def columns(c):
        return pl.ds(c * span, span)

    def cross(k, c):
        at = columns(c)
        return remote(
            part.at[k, 1 - core, :, at], crossed.at[k, :, at], cross_send.at[0], cross_recv.at[k, c], sibling
        )

    strip = 512

    def product_of(k, h, rows_at, at):
        n = pads[h]
        if k == 0:
            return jnp.dot(hidden[h, rows_at, :n], weights[both_rows(2, h), at], preferred_element_type=jnp.float32)
        return jnp.dot(diffs[h, rows_at, : 2 * n], weights[both_rows(0, h, 2), at], preferred_element_type=jnp.float32)

    def partial(k, t, c):
        rows_at = pl.ds(pl.multiple_of(t * slab, slab), slab)
        at = columns(c)
        part[k, t, :, at] = (product_of(k, 0, rows_at, at) + product_of(k, 1, rows_at, at)).astype(jnp.bfloat16)

    routes = ((across, at_across, at_near, chip(x, y, near)), (chip(x, y, near), at_near, at_across, across))
    routed = ((0, 0), (1, 0))
    def join_copy(k, c, n):
        to, theirs, mine, on = routes[routed[k][c]]
        at = columns(c)
        if n == 2:
            source, device = folded.at[k, :, at], on
        else:
            source, device = joined.at[k, (at_both, theirs)[n], :, at], to
        recv = fold_recv.at[k, c] if n == 0 else join_recv.at[k]
        return remote(source, gathered.at[k, n, :, at], join_send.at[0], recv, device)

    def join_start(k, c):
        cross(k, c).wait_recv()
        at = columns(c)
        for n, q in enumerate((at_both, *routes[routed[k][c]][1:3], me)):
            rows_at = pl.ds(pl.multiple_of(q * half, half), half)
            total = part[k, core, rows_at, at].astype(jnp.float32) + crossed[k, rows_at, at].astype(jnp.float32)
            joined[k, q, :, at] = total.astype(jnp.bfloat16)
            if n < 2:
                join_copy(k, c, n).start()

    def join_fold(k, c):
        at = columns(c)
        join_copy(k, c, 0).wait_recv()
        total = gathered[k, 0, :, at].astype(jnp.float32) + joined[k, routes[routed[k][c]][2], :, at].astype(jnp.float32)
        folded[k, :, at] = total.astype(jnp.bfloat16)
        join_copy(k, c, 2).start()

    def stages_in(h):
        for w in range(3):
            stage_in(w, h)

    first_far = (jnp.where(inner, other, far), jnp.where(inner, y, y_flip), jnp.where(inner, 5, 4), 1)
    next_far = (other, jnp.where(inner, y_flip, y), jnp.where(inner, 6, 5), 2)
    last_far = (jnp.where(inner, far, other), y_flip, jnp.where(inner, 4, 6), 2)
    near_own, near_across, far_own = (near, y, 1, 1), (near, y_flip, 2, 2), (far, y, 3, 1)
    lead = (jnp.where(inner, near, far), jnp.where(inner, y, y_flip), jnp.where(inner, 1, 4), 1)
    follow = (jnp.where(inner, other, near), y, jnp.where(inner, 5, 1), 1)
    home = ((z, y, 0, 0), (z, y_flip, 0, 0))
    soon = (near_own, far_own, first_far)
    late = (near_across, next_far, last_far)

    def down_parts(k):
        for c in range(2):
            partial(k, 1 - core, c)
            cross(k, c).start()
        for c in range(2):
            partial(k, core, c)

    for w in range(3):
        turn_in(w)
        if w == 0:
            pl.semaphore_wait(barrier, 9)
        send_stage(0, (w,))
        send_own(0, (w,))
    token_copies[2].wait()
    send_tokens(2, 1)
    send_tokens(2, 0)
    token_copies[0].wait()
    normal(0)
    send_tokens(0, 1)
    send_tokens(0, 0)
    send_own(1)
    token_copies[1].wait()
    normal(1)
    clear_pads()
    for h in range(2):
        keep_own(h)
    for a in range(3):
        keep_tokens(a)
    stages_in(0)
    line_in(0, far_own)
    line_in(0, lead, 0)
    send_others(0)
    send_stage(1)
    tok_in(2, at_across)

    @pl.when(inner)
    def _():
        tok_in(2, at_near)

    line_in(0, follow)

    @pl.when(jnp.logical_not(inner))
    def _():
        tok_in(2, at_near)

    tok_in(0, at_across)
    line_in(1, far_own)

    @pl.when(inner)
    def _():
        tok_in(0, at_near)

    stages_in(1)
    send_tokens(1, 0)
    send_others(1)
    line_in(0, next_far)

    @pl.when(jnp.logical_not(inner))
    def _():
        tok_in(0, at_near)

    send_tokens(1, 1)
    line_in(1, near_own, 0)
    tok_in(2, at_both)
    line_in(0, near_across, 1)
    relayed(2)
    line_in(1, first_far)
    sides_in(0, home)
    project(0, 1, home, True)
    tok_in(0, at_both)
    line_in(1, next_far)
    relayed(0)
    project(0, 0, home, True)
    tok_in(1, at_across)
    sides_in(0, soon)
    project(0, 1, soon)
    line_in(0, last_far)
    project(0, 0, soon)

    @pl.when(inner)
    def _():
        tok_in(1, at_near)

    sides_in(1, home)
    project(1, 0, home, True)
    project(1, 1, home, True)
    line_in(1, near_across, 1)
    line_in(1, last_far)
    sides_in(1, soon)
    project(1, 0, soon)
    project(1, 1, soon)
    sides_in(0, late)
    project(0, 1, late)
    project(0, 0, late)
    back_parts(0)
    grad_make(0)
    grad_out(0)

    @pl.when(jnp.logical_not(inner))
    def _():
        tok_in(1, at_near)

    sides_in(1, late)
    project(1, 0, late)
    project(1, 1, late)
    back_parts(1)
    down_parts(1)
    for c in range(2):
        join_start(1, c)
    grad_make(1)
    grad_out(1)
    tok_in(1, at_both)
    relayed(1)
    project(0, 2, home + soon + late, True)
    fwd_parts(0)
    grad_on(0, 0)
    project(1, 2, home + soon + late, True)
    fwd_parts(1)
    down_parts(0)
    grad_on(0, 1)
    for c in range(2):
        join_start(0, c)
    grad_on(0, 2)
    for c in range(2):
        join_fold(1, c)
    grad_on(0, 3)
    grad_mid(0)
    for n in range(4):
        grad_on(1, n)
    for c in range(2):
        join_fold(0, c)
    grad_mid(1)
    grad_cross(0)
    grad_cross(1)

    mine = pl.ds(pl.multiple_of(core * half, half), half)

    def last(k):
        out = (fwd_out, back_out)[k].at[mine, :]
        return remote(out, out, last_send.at[0], last_recv.at[0], sibling)

    def joined_in(k):
        got(gathered.at[k, pl.ds(1, 2)], join_recv.at[k])

    def total_of(k, at):
        value = joined[k, me, at, :].astype(jnp.float32) + gathered[k, 1, at, :].astype(jnp.float32)
        return value + gathered[k, 2, at, :].astype(jnp.float32)

    tiles = grad_cols.shape[0] // 128
    early = rows * 2 // 128

    def grad_tiles(first, count):
        @pl.loop(0, count)
        def _(n):
            at = pl.ds(pl.multiple_of((first + n) * 128, 128), 128)
            sum_out[:, at] = sum_ref[:, at] + grad_cols[at, :].T

    small = 16

    def out_rows(r):
        return pl.ds(pl.multiple_of(core * half + r * small, small), small)

    sum_copy.wait()
    grad_tiles(y * (tiles - early), early)
    joined_in(0)
    for r in range(half // small):
        fwd_out[out_rows(r), :] = (0.5 * total_of(0, pl.ds(r * small, small))).astype(jnp.bfloat16)
    last(0).start()
    joined_in(1)
    for r in range(half // small):
        values = tokens_ref[out_rows(r), :].astype(jnp.float32)
        factor = lax.rsqrt(jnp.mean(values * values, axis=-1, keepdims=True) + norm_eps)
        scaled = total_of(1, pl.ds(r * small, small)) * gain_ref[...]
        cubed = factor * factor * factor
        back_out[out_rows(r), :] = (
            factor * scaled - values * cubed * jnp.mean(scaled * values, axis=-1, keepdims=True)
        ).astype(jnp.bfloat16)
    last(1).start()

    for h in range(2):
        grad_in(h)
    grad_tiles((1 - y) * early, tiles - early)

    gone(weights.at[pl.ds(0, 3 * rows), pl.ds(0, 14 * depth)], block_send.at[0])

    @pl.when(inner)
    def _():
        gone(weights.at[pl.ds(0, 3 * rows), pl.ds(0, 4 * depth)], inner_send.at[0])

    gone(toks.at[:, pl.ds(0, 6 * half), :], tok_send.at[0])
    gone(grad_side, gside_send.at[0])
    gone(grad_total, gsend.at[0])
    gone(part.at[0], cross_send.at[0])
    gone(joined.at[:, pl.ds(0, 3)], join_send.at[0])
    gone(fwd_out, last_send.at[0])
    got(fwd_out, last_recv.at[0])


def fused_shards(
    split, fwd_tokens, back_tokens, out_grad, norm_gain, gate_weight, up_weight, down_weight, gate_grad_sum
):
    tokens, width = fwd_tokens.shape
    depth, cols = gate_weight.shape
    rows = cols // 4
    out_bytes = 2 * tokens * width * 2 + depth * cols * 4
    wide = max(padded(split), padded(rows - split))
    held = 3 * (padded(split) + padded(rows - split))
    half = tokens // 2
    slab = half * 4
    narrow, full = jnp.bfloat16, jnp.float32
    dma = pltpu.SemaphoreType.DMA
    vmem = pl.BlockSpec(memory_space=pltpu.VMEM)
    hbm = pl.BlockSpec(memory_space=pl.ANY)
    return pl.pallas_call(
        functools.partial(layer_kernel, split),
        out_shape=(
            pltpu.VMEM((tokens, width), narrow),
            pltpu.VMEM((tokens, width), narrow),
            pltpu.VMEM((depth, cols), full),
        ),
        in_specs=[hbm] * 3 + [vmem] + [hbm] * 4,
        out_specs=(vmem,) * 3,
        scratch_shapes=[
            pltpu.VMEM((3, depth, cols), narrow),
            pltpu.VMEM((3, tokens, width), narrow),
            pltpu.VMEM((depth, cols), full),
            pltpu.VMEM((3, cols, depth), narrow),
            pltpu.VMEM((2, tokens, width), narrow),
            pltpu.VMEM((3, 2 * slab, width), narrow),
            pltpu.VMEM((held, width), narrow),
            pltpu.VMEM((held, depth), narrow),
            pltpu.VMEM((2, 2 * slab, 2 * wide), full),
            pltpu.VMEM((2, 2 * slab, wide), full),
            pltpu.VMEM((2, 2 * slab, 2 * wide), full),
            pltpu.VMEM((2, 2 * slab, wide), narrow),
            pltpu.VMEM((2, 2 * slab, 2 * wide), narrow),
            pltpu.VMEM((2, 2 * slab, wide), narrow),
            pltpu.VMEM((2, 2, slab, width), narrow),
            pltpu.VMEM((2, slab, width), narrow),
            pltpu.VMEM((2, 4, half, width), narrow),
            pltpu.VMEM((2, half, width), narrow),
            pltpu.VMEM((2, 3, half, width), narrow),
            pltpu.VMEM((2, 8, rows, depth), narrow),
            pltpu.VMEM((8, rows, depth), narrow),
            pltpu.VMEM((8, rows, depth), narrow),
            pltpu.VMEM((2, rows, depth), narrow),
            pltpu.VMEM((3, 2, rows, depth), narrow),
            pltpu.VMEM((2, rows, depth), narrow),
            pltpu.VMEM((2, rows, depth), narrow),
            pltpu.VMEM((cols, depth), full),
            dma((1,)),
            dma((1,)),
            dma((4, 7)),
            dma((4,)),
            dma((2, 3)),
            dma((1,)),
            dma((3, 6)),
            dma((3,)),
            dma((1,)),
            dma((2, 4)),
            dma((1,)),
            dma((2, 3)),
            dma((2,)),
            dma((2,)),
            dma((1,)),
            dma((2, 2)),
            dma((1,)),
            dma((2, 2)),
            dma((2,)),
            dma((1,)),
            dma((1,)),
            dma((3,)),
            dma((3,)),
            dma((1,)),
        ],
        compiler_params=pltpu.CompilerParams(
            collective_id=0, has_side_effects=True, vmem_limit_bytes=vmem_bytes - out_bytes
        ),
    )(
        fwd_tokens, back_tokens, out_grad, norm_gain.reshape(1, width),
        gate_weight, up_weight, down_weight, gate_grad_sum,
    )


def body_for(mesh):
    def body(*args):
        tokens, width = args[0].shape
        depth, cols = args[4].shape
        rows = cols // 4
        fits = (
            mesh.shape["tp"] == 2 and mesh.shape["fs"] == 16
            and depth == 128 and width == 16 * depth and cols % 128 == 0 and tokens % 128 == 0
            and rows > 256 and rows % 16 == 0
        )
        if not fits:
            return shards(*args)
        return fused_shards((rows - 1) // 256 * 256, *args)

    return body


def solution(mesh):
    in_specs = (
        P("fs", None),
        P("fs", None),
        P("fs", None),
        P(),
        P("fs", "tp"),
        P("fs", "tp"),
        P("fs", "tp"),
        P("fs", "tp"),
    )
    out_specs = (P("fs", None), P("fs", None), P("fs", "tp"))
    return jax.shard_map(body_for(mesh), mesh=mesh, in_specs=in_specs, out_specs=out_specs, check_vma=False)
```

```python
import functools

import jax
import jax.numpy as jnp
from jax import lax
from jax.experimental import pallas as pl
from jax.experimental.pallas import tpu as pltpu
from jax.sharding import PartitionSpec as P

norm_eps = 0.25
vmem_bytes = 66_900_000


def normalize(tokens, norm_gain):
    values = tokens.astype(jnp.float32)
    factor = lax.rsqrt(jnp.mean(values * values, axis=-1, keepdims=True) + norm_eps)
    return (values, factor, (values * factor * norm_gain).astype(jnp.bfloat16))


def shards(
    fwd_tokens, back_tokens, out_grad, norm_gain, gate_weight, up_weight, down_weight, gate_grad_sum
):
    fwd_normed = normalize(fwd_tokens, norm_gain)[2]
    columns = fwd_normed
    gate_pre = jnp.dot(
        columns,
        lax.all_gather(gate_weight, "fs", axis=0, tiled=True),
        preferred_element_type=jnp.float32,
    )
    up_pre = jnp.dot(
        columns,
        lax.all_gather(up_weight, "fs", axis=0, tiled=True),
        preferred_element_type=jnp.float32,
    )
    hidden = (gate_pre * jax.nn.sigmoid(gate_pre) * up_pre).astype(jnp.bfloat16)
    partial_value = jnp.dot(
        hidden,
        lax.all_gather(down_weight, "fs", axis=0, tiled=True).T,
        preferred_element_type=jnp.float32,
    )
    summed = lax.psum(partial_value.astype(jnp.bfloat16), "tp").astype(jnp.float32)
    fwd_out = (0.5 * summed).astype(jnp.bfloat16)
    gate_whole = lax.all_gather(gate_weight, "fs", axis=0, tiled=True)
    up_whole = lax.all_gather(up_weight, "fs", axis=0, tiled=True)
    down_whole = lax.all_gather(down_weight, "fs", axis=0, tiled=True)
    values, factor, back_normed = normalize(back_tokens, norm_gain)
    gate_pre = jnp.dot(back_normed, gate_whole, preferred_element_type=jnp.float32)
    up_pre = jnp.dot(back_normed, up_whole, preferred_element_type=jnp.float32)
    sigmoid_gate = jax.nn.sigmoid(gate_pre)
    back_hidden = 0.5 * jnp.dot(out_grad, down_whole, preferred_element_type=jnp.float32)
    gate_diff = (
        back_hidden * up_pre * sigmoid_gate * (1.0 + gate_pre * (1.0 - sigmoid_gate))
    ).astype(jnp.bfloat16)
    up_diff = (back_hidden * gate_pre * sigmoid_gate).astype(jnp.bfloat16)
    columns = back_normed
    gate_grad_out = gate_grad_sum + lax.psum_scatter(
        jnp.dot(columns.T, gate_diff, preferred_element_type=jnp.float32),
        "fs",
        scatter_dimension=0,
        tiled=True,
    )
    partial_diff = jnp.dot(gate_diff, gate_whole.T, preferred_element_type=jnp.float32)
    partial_diff = partial_diff + jnp.dot(up_diff, up_whole.T, preferred_element_type=jnp.float32)
    normed_diff = lax.psum(partial_diff.astype(jnp.bfloat16), "tp").astype(jnp.float32)
    scaled = normed_diff * norm_gain
    cubed = factor * factor * factor
    back_grad = (
        factor * scaled - values * cubed * jnp.mean(scaled * values, axis=-1, keepdims=True)
    ).astype(jnp.bfloat16)
    back_grad, gate_grad_out = (back_grad, gate_grad_out)
    return (fwd_out, back_grad, gate_grad_out)


MESH = pl.DeviceIdType.MESH


def wide_dot(a, b):
    return lax.dot_general(a, b, (((1,), (1,)), ((), ())), preferred_element_type=jnp.float32)


def padded(size):
    return (size + 127) // 128 * 128


def layer_kernel(
    split, fwd_in, tokens_in, grad_in_ref, gain_ref, gate_in, up_in, down_in, sum_in,
    fwd_out, back_out, sum_out,
    raw, raw_tokens, sum_ref, turned, normed, toks, weights, staged, back_acc, down_acc, fwd_acc, hidden, diffs, diff_cols,
    part, crossed, joined, folded, gathered, grad_send, grad_side, grad_total, grad_pass, grad_recv, grad_turn, turn_recv, grad_cols,
    block_send, inner_send, line_recv, held_recv, side_recv, tok_send, tok_recv, relay_recv,
    gside_send, gside_recv, gsend, glev_recv, gpass_recv, gturn_recv,
    cross_send, cross_recv, join_send, fold_recv, join_recv, last_send, last_recv, raw_sem, token_sem, sum_sem,
):
    fs, core = lax.axis_index("fs"), lax.axis_index("tp")
    x, y, z = fs % 2, fs // 2 % 2, fs // 4
    odd = z % 2
    inner = jnp.logical_and(z > 0, z < 3)
    near, far, other = z + 1 - 2 * odd, (z + 2) % 4, 3 - z
    sibling = (fs, 1 - core)
    rows = turned.shape[1] // 4
    starts, sizes = (0, split), (split, rows - split)
    pads = tuple(padded(size) for size in sizes)
    depth = gate_in.shape[0]
    half = fwd_in.shape[0] // 2
    tokens_ref, fwd_ref, grad_ref = raw_tokens.at[0], raw_tokens.at[1], raw_tokens.at[2]
    slab = half * 4
    width = fwd_in.shape[1]
    band = 4 * depth

    def chip(to_x, to_y, to_z):
        return (to_z * 4 + to_y * 2 + to_x, core)

    beside, across = chip(1 - x, y, z), chip(x, 1 - y, z)
    y_flip = 1 - y

    barrier = pltpu.get_barrier_semaphore()
    for device in (
        sibling, beside, across, chip(x, y, near), chip(x, y, far), chip(x, y, other),
        chip(x, 1 - y, near), chip(x, 1 - y, far), chip(x, 1 - y, other),
    ):
        pl.semaphore_signal(barrier, inc=1, device_id=device, device_id_type=MESH)

    raw_copies = [pltpu.make_async_copy(ref, raw.at[w], raw_sem.at[w]) for w, ref in enumerate((gate_in, up_in, down_in))]
    token_copies = [
        pltpu.make_async_copy(ref, raw_tokens.at[a], token_sem.at[a]) for a, ref in enumerate((tokens_in, fwd_in, grad_in_ref))
    ]
    sum_copy = pltpu.make_async_copy(sum_in, sum_ref, sum_sem.at[0])
    for copy in (*raw_copies, token_copies[2], token_copies[0], token_copies[1], sum_copy):
        copy.start()

    def turn_in(w):
        raw_copies[w].wait()
        for n in range(turned.shape[1] // 128):
            at = pl.ds(n * 128, 128)
            turned[w, at, :] = raw[w, :, at].T

    def remote(src, dst, send, recv, device):
        return pltpu.make_async_remote_copy(
            src_ref=src, dst_ref=dst, send_sem=send, recv_sem=recv, device_id=device, device_id_type=MESH
        )

    def got(ref, sem):
        remote(ref, ref, sem, sem, sibling).wait_recv()

    def gone(ref, sem):
        remote(ref, ref, sem, sem, sibling).wait_send()

    def own_rows(h, to_y, to_odd):
        return pl.ds(pl.multiple_of((to_y * 2 + to_odd) * rows + starts[h], 16), sizes[h])

    def held_rows(w, h):
        return pl.ds(3 * starts[h] + w * pads[h], sizes[h])

    def both_rows(w, h, count=1):
        return pl.ds(3 * starts[h] + w * pads[h], count * pads[h])

    def own(w, h, to_y, to_odd):
        return turned.at[w, own_rows(h, to_y, to_odd), :]

    def lanes(src):
        return pl.ds(pl.multiple_of(src * depth, depth), depth)

    def level_lanes(s):
        return pl.ds(pl.multiple_of(s * band, band), band)

    def block(w, h, src):
        return weights.at[held_rows(w, h), lanes(src)]

    def send_block(w, h, src, source, device, recv, send):
        return remote(source, block(w, h, src), send.at[0], recv, device)

    def line_sem(w, h, role):
        return line_recv.at[w if h == 0 else 3, role]

    def held_sem(w, h):
        return held_recv.at[w if h == 0 else 3]

    def block_in(w, h, sem):
        if h == 0:
            got(weights.at[pl.ds(0, sizes[0]), pl.ds(0, depth)], sem)
        elif w == 0:
            got(weights.at[pl.ds(0, 3 * sizes[1]), pl.ds(0, depth)], sem)

    def to_near(w, h, src, source, line):
        send_block(w, h, src, source, chip(x, y, near), line_sem(w, h, 1 + line), block_send).start()

    def to_far(w, h, src, source, line):
        send_block(w, h, src, source, chip(x, y, far), line_sem(w, h, 3 + line), block_send).start()

    def to_other(w, h, src, source, line):
        @pl.when(inner)
        def _():
            send_block(w, h, src, source, chip(x, y, other), line_sem(w, h, 5 + line), inner_send).start()

    def pass_far(w, h, src, source, line):
        @pl.when(inner)
        def _():
            send_block(w, h, src, source, chip(x, y, far), line_sem(w, h, 5 + line), inner_send).start()

    def side(w, h, src, source, bundle):
        send_block(w, h, src, source, beside, side_recv.at[h, bundle], block_send).start()

    def send_stage(h, some=range(3)):
        for w in some:
            send_block(w, h, fs, own(w, h, 1 - y, odd), across, line_sem(w, h, 0), block_send).start()
            remote(
                own(w, h, 1 - y, 1 - odd), staged.at[held_rows(w, h), :], block_send.at[0], held_sem(w, h), across
            ).start()

    def send_own(h, some=range(3)):
        for w in some:
            to_near(w, h, fs, own(w, h, y, 1 - odd), 0)
            to_far(w, h, fs, own(w, h, y, odd), 0)
            side(w, h, fs, own(w, h, y, odd), 0)

    def send_others(h):
        for w in range(3):
            to_other(w, h, fs, own(w, h, y, 1 - odd), 0)
        for w in range(3):
            to_other(w, h, z * 4 + (1 - y) * 2 + x, staged.at[held_rows(w, h), :], 1)

    def keep_own(h):
        for w in range(3):
            weights[held_rows(w, h), lanes(fs)] = turned[w, own_rows(h, y, odd), :]

    def clear_pads():
        for h in range(2):
            if pads[h] > sizes[h]:
                for w in range(3):
                    gap = pl.ds(3 * starts[h] + w * pads[h] + sizes[h], pads[h] - sizes[h])
                    weights[gap, :] = jnp.zeros((pads[h] - sizes[h], width), jnp.bfloat16)

    def stage_in(w, h):
        src = z * 4 + (1 - y) * 2 + x
        held = staged.at[held_rows(w, h), :]
        block_in(w, h, held_sem(w, h))
        to_near(w, h, src, held, 1)
        block_in(w, h, line_sem(w, h, 0))
        to_far(w, h, src, block(w, h, src), 1)
        side(w, h, src, block(w, h, src), 0)

    def line_in(h, group, passed=None):
        s, line, role, bundle = group
        for w in range(3):
            src = s * 4 + line * 2 + x
            block_in(w, h, line_sem(w, h, role))
            if passed is not None:
                pass_far(w, h, src, block(w, h, src), passed)
            side(w, h, src, block(w, h, src), bundle)

    def sides_in(h, groups):
        got(weights.at[pl.ds(0, 3 * sizes[h]), pl.ds(0, len(groups) * depth)], side_recv.at[h, groups[0][3]])

    me = y * 2 + odd
    at_near, at_across, at_both = y * 2 + 1 - odd, (1 - y) * 2 + odd, (1 - y) * 2 + 1 - odd

    def token_rows(a, at):
        return grad_ref.at[at, :] if a == 2 else normed.at[a, at, :]

    def tok_block(a, h, q, n=None):
        rows_of = half if n is None else half // 2
        first = h * slab + q * half + (0 if n is None else n * rows_of)
        return toks.at[a, pl.ds(pl.multiple_of(first, rows_of), rows_of), :]

    def tok_copy(a, q, source, device, role, n=None):
        return remote(source, tok_block(a, core, q, n), tok_send.at[0], tok_recv.at[a, role], device)

    def relay(a, q, n=None):
        block_of = tok_block(a, core, q, n)
        return remote(block_of, block_of, tok_send.at[0], relay_recv.at[a], sibling)

    def tok_pieces(a):
        return (None,) if a != 1 else (0, 1)

    def send_tokens(a, role):
        for n in tok_pieces(a) if role == 0 else (None,):
            rows_of = half if n is None else half // 2
            mine = token_rows(a, pl.ds(pl.multiple_of(core * half + (n or 0) * rows_of, rows_of), rows_of))
            tok_copy(a, me, mine, (chip(x, y, near), across)[role], role + 3 * (n or 0), n).start()

    def normal(a):
        @pl.loop(0, tokens_ref.shape[0] // 16)
        def _(r):
            at = pl.ds(pl.multiple_of(r * 16, 16), 16)
            normed[a, at, :] = normalize((tokens_ref, fwd_ref)[a][at, :], gain_ref[...])[2]

    def keep_tokens(a):
        for h in range(2):
            toks[a, pl.ds(pl.multiple_of(h * slab + me * half, half), half), :] = token_rows(a, pl.ds(h * half, half))[...]

    def tok_in(a, q):
        role = [q is at for at in (at_near, at_across, at_both)].index(True)
        for n in tok_pieces(a) if role != 1 else (None,):
            got(tok_block(a, core, q, n), tok_recv.at[a, role + 3 * (n or 0)])
            if role == 0:
                tok_copy(a, q, tok_block(a, core, q, n), across, 2 + 3 * (n or 0), n).start()
            relay(a, q, n).start()

    def relayed(a):
        got(toks.at[a, pl.ds(0, 3 * half), :], relay_recv.at[a])

    def project(h, kind, groups, first=False):
        a, w, count, into = ((0, 0, 2, back_acc), (2, 2, 1, down_acc), (1, 0, 2, fwd_acc))[kind]
        wide = count * pads[h]
        at_rows = both_rows(w, h, count)
        for t in range(2):
            at_tokens = pl.ds(t * slab, slab)
            value = None if first else into[h, at_tokens, :wide]
            for s, line, _, _ in groups:
                at = pl.ds(pl.multiple_of((s * 4 + line * 2) * depth, 2 * depth), 2 * depth)
                term = wide_dot(toks[a, at_tokens, at], weights[at_rows, at])
                value = term if value is None else value + term
            into[h, at_tokens, :wide] = value

    piece = 64

    def back_parts(h):
        n = pads[h]

        @pl.loop(0, 2 * slab // piece)
        def _(r):
            at = pl.ds(pl.multiple_of(r * piece, piece), piece)
            gate, up = back_acc[h, at, :n], back_acc[h, at, n : 2 * n]
            s = jax.nn.sigmoid(gate)
            back = 0.5 * down_acc[h, at, :n]
            gate_diff = (back * up * s * (1.0 + gate * (1.0 - s))).astype(jnp.bfloat16)
            diff_cols[h, at, :n] = gate_diff
            diffs[h, at, :n] = gate_diff
            diffs[h, at, n : 2 * n] = (back * gate * s).astype(jnp.bfloat16)

    def fwd_parts(h):
        n = pads[h]

        @pl.loop(0, 2 * slab // piece)
        def _(r):
            at = pl.ds(pl.multiple_of(r * piece, piece), piece)
            gate, up = fwd_acc[h, at, :n], fwd_acc[h, at, n : 2 * n]
            hidden[h, at, :n] = (gate * jax.nn.sigmoid(gate) * up).astype(jnp.bfloat16)

    def grad_rows(h):
        return pl.ds(starts[h], sizes[h])

    def grad_across(h, n):
        pair = pl.ds((other, far, near, z)[n] * 2, 2)
        return remote(
            grad_send.at[1 - x, pair, grad_rows(h)], grad_side.at[pair, grad_rows(h)], gside_send.at[0], gside_recv.at[h, n], beside
        )

    def grad_make(h):
        diff_turned = diff_cols[h, :, : sizes[h]].T
        for s in range(4):
            at = level_lanes(s)
            product = jnp.dot(diff_turned, toks[0, :, at], preferred_element_type=jnp.float32)
            product = product.astype(jnp.bfloat16)
            for q in range(4):
                grad_send[q % 2, s * 2 + q // 2, grad_rows(h), :] = product[:, q * depth : (q + 1) * depth]

    def grad_out(h):
        for s in range(4):
            grad_across(h, s).start()

    def grad_to(h, n):
        s = (near, far, other)[n]
        source = grad_total.at[pl.ds(s * 2, 2), grad_rows(h)]
        return remote(source, grad_recv.at[n, :, grad_rows(h)], gsend.at[0], glev_recv.at[h, n], chip(x, y, s))

    def grad_past(h):
        source = grad_total.at[pl.ds(other * 2, 2), grad_rows(h)]
        return remote(source, grad_pass.at[:, grad_rows(h)], gsend.at[0], gpass_recv.at[h], chip(x, y, far))

    def grad_turned(h):
        return remote(
            grad_turn.at[:, grad_rows(h)], turn_recv.at[:, grad_rows(h)], gsend.at[0], gturn_recv.at[h], across
        )

    def grad_on(h, n):
        grad_across(h, n).wait_recv()
        for line in range(2):
            j = (other, far, near, z)[n] * 2 + line
            total = grad_send[x, j, grad_rows(h), :].astype(jnp.float32) + grad_side[j, grad_rows(h), :].astype(jnp.float32)
            grad_total[j, grad_rows(h), :] = total.astype(jnp.bfloat16)
        if n == 0:

            @pl.when(inner)
            def _():
                grad_to(h, 2).start()

            @pl.when(jnp.logical_not(inner))
            def _():
                grad_past(h).start()

        if n == 1:
            grad_to(h, 1).start()
        if n == 2:

            @pl.when(jnp.logical_not(inner))
            def _():
                grad_to(h, 0).start()

    def grad_mid(h):
        @pl.when(inner)
        def _():
            grad_past(h).wait_recv()
            for line in range(2):
                j = near * 2 + line
                total = grad_total[j, grad_rows(h), :].astype(jnp.float32) + grad_pass[line, grad_rows(h), :].astype(jnp.float32)
                grad_total[j, grad_rows(h), :] = total.astype(jnp.bfloat16)
            grad_to(h, 0).start()

    def grad_cols_at(h, to_y, to_odd):
        return pl.ds(pl.multiple_of((to_y * 2 + to_odd) * rows + starts[h], 16), sizes[h])

    def grad_cross(h):
        at = grad_rows(h)
        for n in range(2):
            grad_to(h, n).wait_recv()

        @pl.when(inner)
        def _():
            grad_to(h, 2).wait_recv()
            for line in range(2):
                total = grad_recv[0, line, at, :].astype(jnp.float32) + grad_recv[2, line, at, :].astype(jnp.float32)
                grad_recv[0, line, at, :] = total.astype(jnp.bfloat16)

        def sums(line):
            same = grad_total[z * 2 + line, at, :].astype(jnp.float32) + grad_recv[1, line, at, :].astype(jnp.float32)
            return same, grad_recv[0, line, at, :]

        same, unlike = sums(1 - y)
        grad_turn[0, at, :] = same.astype(jnp.bfloat16)
        grad_turn[1, at, :] = unlike
        grad_turned(h).start()
        same, unlike = sums(y)
        grad_cols[grad_cols_at(h, y, odd), :] = same
        grad_cols[grad_cols_at(h, y, 1 - odd), :] = unlike.astype(jnp.float32)

    def grad_in(h):
        grad_turned(h).wait_recv()
        for n, to_odd in enumerate((odd, 1 - odd)):
            grad_cols[grad_cols_at(h, 1 - y, to_odd), :] = turn_recv[n, grad_rows(h), :].astype(jnp.float32)

    span = width // 2

    def columns(c):
        return pl.ds(c * span, span)

    def cross(k, c):
        at = columns(c)
        return remote(
            part.at[k, 1 - core, :, at], crossed.at[k, :, at], cross_send.at[0], cross_recv.at[k, c], sibling
        )

    strip = 512

    def product_of(k, h, rows_at, at):
        n = pads[h]
        if k == 0:
            return jnp.dot(hidden[h, rows_at, :n], weights[both_rows(2, h), at], preferred_element_type=jnp.float32)
        return jnp.dot(diffs[h, rows_at, : 2 * n], weights[both_rows(0, h, 2), at], preferred_element_type=jnp.float32)

    def partial(k, t, c):
        rows_at = pl.ds(pl.multiple_of(t * slab, slab), slab)
        at = columns(c)
        part[k, t, :, at] = (product_of(k, 0, rows_at, at) + product_of(k, 1, rows_at, at)).astype(jnp.bfloat16)

    routes = ((across, at_across, at_near, chip(x, y, near)), (chip(x, y, near), at_near, at_across, across))
    routed = ((0, 0), (1, 0))
    def join_copy(k, c, n):
        to, theirs, mine, on = routes[routed[k][c]]
        at = columns(c)
        if n == 2:
            source, device = folded.at[k, :, at], on
        else:
            source, device = joined.at[k, (at_both, theirs)[n], :, at], to
        recv = fold_recv.at[k, c] if n == 0 else join_recv.at[k]
        return remote(source, gathered.at[k, n, :, at], join_send.at[0], recv, device)

    def join_start(k, c):
        if c == 0:
            return
        for c in range(2):
            cross(k, c).wait_recv()
        for n in range(4):
            for c in range(2):
                at = columns(c)
                q = (at_both, *routes[routed[k][c]][1:3], me)[n]
                rows_at = pl.ds(pl.multiple_of(q * half, half), half)
                total = part[k, core, rows_at, at].astype(jnp.float32) + crossed[k, rows_at, at].astype(jnp.float32)
                joined[k, q, :, at] = total.astype(jnp.bfloat16)
                if n < 2:
                    join_copy(k, c, n).start()

    def join_fold(k, c):
        at = columns(c)
        join_copy(k, c, 0).wait_recv()
        total = gathered[k, 0, :, at].astype(jnp.float32) + joined[k, routes[routed[k][c]][2], :, at].astype(jnp.float32)
        folded[k, :, at] = total.astype(jnp.bfloat16)
        join_copy(k, c, 2).start()

    def stages_in(h):
        for w in range(3):
            stage_in(w, h)

    first_far = (jnp.where(inner, other, far), jnp.where(inner, y, y_flip), jnp.where(inner, 5, 4), 1)
    next_far = (other, jnp.where(inner, y_flip, y), jnp.where(inner, 6, 5), 2)
    last_far = (jnp.where(inner, far, other), y_flip, jnp.where(inner, 4, 6), 2)
    near_own, near_across, far_own = (near, y, 1, 1), (near, y_flip, 2, 2), (far, y, 3, 1)
    lead = (jnp.where(inner, near, far), jnp.where(inner, y, y_flip), jnp.where(inner, 1, 4), 1)
    follow = (jnp.where(inner, other, near), y, jnp.where(inner, 5, 1), 1)
    home = ((z, y, 0, 0), (z, y_flip, 0, 0))
    soon = (near_own, far_own, first_far)
    late = (near_across, next_far, last_far)

    def down_parts(k):
        for c in range(2):
            partial(k, 1 - core, c)
            cross(k, c).start()
        for c in range(2):
            partial(k, core, c)

    for w in range(3):
        turn_in(w)
        if w == 0:
            pl.semaphore_wait(barrier, 9)
        send_stage(0, (w,))
        send_own(0, (w,))
    token_copies[2].wait()
    send_tokens(2, 1)
    send_tokens(2, 0)
    token_copies[0].wait()
    normal(0)
    send_tokens(0, 1)
    send_tokens(0, 0)
    send_own(1)
    token_copies[1].wait()
    normal(1)
    clear_pads()
    for h in range(2):
        keep_own(h)
    for a in range(3):
        keep_tokens(a)
    stages_in(0)
    line_in(0, far_own)
    line_in(0, lead, 0)
    send_others(0)
    send_stage(1)
    tok_in(2, at_across)

    @pl.when(inner)
    def _():
        tok_in(2, at_near)

    line_in(0, follow)

    @pl.when(jnp.logical_not(inner))
    def _():
        tok_in(2, at_near)

    tok_in(0, at_across)
    line_in(1, far_own)

    @pl.when(inner)
    def _():
        tok_in(0, at_near)

    stages_in(1)
    send_tokens(1, 0)
    send_others(1)
    line_in(0, next_far)

    @pl.when(jnp.logical_not(inner))
    def _():
        tok_in(0, at_near)

    send_tokens(1, 1)
    line_in(1, near_own, 0)
    tok_in(2, at_both)
    line_in(0, near_across, 1)
    relayed(2)
    line_in(1, first_far)
    sides_in(0, home)
    project(0, 1, home, True)
    tok_in(0, at_both)
    line_in(1, next_far)
    relayed(0)
    project(0, 0, home, True)
    tok_in(1, at_across)
    sides_in(0, soon)
    project(0, 1, soon)
    line_in(0, last_far)
    project(0, 0, soon)

    @pl.when(inner)
    def _():
        tok_in(1, at_near)

    sides_in(1, home)
    project(1, 0, home, True)
    project(1, 1, home, True)
    line_in(1, near_across, 1)
    line_in(1, last_far)
    sides_in(1, soon)
    project(1, 0, soon)
    project(1, 1, soon)
    sides_in(0, late)
    project(0, 1, late)
    project(0, 0, late)
    back_parts(0)
    grad_make(0)
    grad_out(0)

    @pl.when(jnp.logical_not(inner))
    def _():
        tok_in(1, at_near)

    sides_in(1, late)
    project(1, 0, late)
    project(1, 1, late)
    back_parts(1)
    down_parts(1)
    for c in range(2):
        join_start(1, c)
    tok_in(1, at_both)
    grad_on(0, 0)
    relayed(1)
    project(0, 2, home + soon + late, True)
    fwd_parts(0)
    grad_on(0, 1)
    project(1, 2, home + soon + late, True)
    fwd_parts(1)
    down_parts(0)
    grad_on(0, 2)
    for c in range(2):
        join_start(0, c)
    grad_make(1)
    grad_out(1)
    for c in range(2):
        join_fold(1, c)
    grad_on(0, 3)
    grad_mid(0)
    for n in range(4):
        grad_on(1, n)
    for c in range(2):
        join_fold(0, c)
    grad_mid(1)
    grad_cross(0)
    grad_cross(1)

    mine = pl.ds(pl.multiple_of(core * half, half), half)

    def last(k):
        out = (fwd_out, back_out)[k].at[mine, :]
        return remote(out, out, last_send.at[0], last_recv.at[0], sibling)

    def joined_in(k):
        got(gathered.at[k, pl.ds(1, 2)], join_recv.at[k])

    def total_of(k, at):
        value = joined[k, me, at, :].astype(jnp.float32) + gathered[k, 1, at, :].astype(jnp.float32)
        return value + gathered[k, 2, at, :].astype(jnp.float32)

    tiles = grad_cols.shape[0] // 128
    early = rows * 2 // 128

    def grad_tiles(first, count):
        @pl.loop(0, count)
        def _(n):
            at = pl.ds(pl.multiple_of((first + n) * 128, 128), 128)
            sum_out[:, at] = sum_ref[:, at] + grad_cols[at, :].T

    small = 16

    def out_rows(r):
        return pl.ds(pl.multiple_of(core * half + r * small, small), small)

    sum_copy.wait()
    grad_tiles(y * (tiles - early), early)
    joined_in(0)
    for r in range(half // small):
        fwd_out[out_rows(r), :] = (0.5 * total_of(0, pl.ds(r * small, small))).astype(jnp.bfloat16)
    last(0).start()
    joined_in(1)
    for r in range(half // small):
        values = tokens_ref[out_rows(r), :].astype(jnp.float32)
        factor = lax.rsqrt(jnp.mean(values * values, axis=-1, keepdims=True) + norm_eps)
        scaled = total_of(1, pl.ds(r * small, small)) * gain_ref[...]
        cubed = factor * factor * factor
        back_out[out_rows(r), :] = (
            factor * scaled - values * cubed * jnp.mean(scaled * values, axis=-1, keepdims=True)
        ).astype(jnp.bfloat16)
    last(1).start()

    for h in range(2):
        grad_in(h)
    grad_tiles((1 - y) * early, tiles - early)

    gone(weights.at[pl.ds(0, 3 * rows), pl.ds(0, 14 * depth)], block_send.at[0])

    @pl.when(inner)
    def _():
        gone(weights.at[pl.ds(0, 3 * rows), pl.ds(0, 4 * depth)], inner_send.at[0])

    gone(toks.at[:, pl.ds(0, 6 * half), :], tok_send.at[0])
    gone(grad_side, gside_send.at[0])
    gone(grad_total, gsend.at[0])
    gone(part.at[0], cross_send.at[0])
    gone(joined.at[:, pl.ds(0, 3)], join_send.at[0])
    gone(fwd_out, last_send.at[0])
    got(fwd_out, last_recv.at[0])


def fused_shards(
    split, fwd_tokens, back_tokens, out_grad, norm_gain, gate_weight, up_weight, down_weight, gate_grad_sum
):
    tokens, width = fwd_tokens.shape
    depth, cols = gate_weight.shape
    rows = cols // 4
    out_bytes = 2 * tokens * width * 2 + depth * cols * 4
    wide = max(padded(split), padded(rows - split))
    held = 3 * (padded(split) + padded(rows - split))
    half = tokens // 2
    slab = half * 4
    narrow, full = jnp.bfloat16, jnp.float32
    dma = pltpu.SemaphoreType.DMA
    vmem = pl.BlockSpec(memory_space=pltpu.VMEM)
    hbm = pl.BlockSpec(memory_space=pl.ANY)
    return pl.pallas_call(
        functools.partial(layer_kernel, split),
        out_shape=(
            pltpu.VMEM((tokens, width), narrow),
            pltpu.VMEM((tokens, width), narrow),
            pltpu.VMEM((depth, cols), full),
        ),
        in_specs=[hbm] * 3 + [vmem] + [hbm] * 4,
        out_specs=(vmem,) * 3,
        scratch_shapes=[
            pltpu.VMEM((3, depth, cols), narrow),
            pltpu.VMEM((3, tokens, width), narrow),
            pltpu.VMEM((depth, cols), full),
            pltpu.VMEM((3, cols, depth), narrow),
            pltpu.VMEM((2, tokens, width), narrow),
            pltpu.VMEM((3, 2 * slab, width), narrow),
            pltpu.VMEM((held, width), narrow),
            pltpu.VMEM((held, depth), narrow),
            pltpu.VMEM((2, 2 * slab, 2 * wide), full),
            pltpu.VMEM((2, 2 * slab, wide), full),
            pltpu.VMEM((2, 2 * slab, 2 * wide), full),
            pltpu.VMEM((2, 2 * slab, wide), narrow),
            pltpu.VMEM((2, 2 * slab, 2 * wide), narrow),
            pltpu.VMEM((2, 2 * slab, wide), narrow),
            pltpu.VMEM((2, 2, slab, width), narrow),
            pltpu.VMEM((2, slab, width), narrow),
            pltpu.VMEM((2, 4, half, width), narrow),
            pltpu.VMEM((2, half, width), narrow),
            pltpu.VMEM((2, 3, half, width), narrow),
            pltpu.VMEM((2, 8, rows, depth), narrow),
            pltpu.VMEM((8, rows, depth), narrow),
            pltpu.VMEM((8, rows, depth), narrow),
            pltpu.VMEM((2, rows, depth), narrow),
            pltpu.VMEM((3, 2, rows, depth), narrow),
            pltpu.VMEM((2, rows, depth), narrow),
            pltpu.VMEM((2, rows, depth), narrow),
            pltpu.VMEM((cols, depth), full),
            dma((1,)),
            dma((1,)),
            dma((4, 7)),
            dma((4,)),
            dma((2, 3)),
            dma((1,)),
            dma((3, 6)),
            dma((3,)),
            dma((1,)),
            dma((2, 4)),
            dma((1,)),
            dma((2, 3)),
            dma((2,)),
            dma((2,)),
            dma((1,)),
            dma((2, 2)),
            dma((1,)),
            dma((2, 2)),
            dma((2,)),
            dma((1,)),
            dma((1,)),
            dma((3,)),
            dma((3,)),
            dma((1,)),
        ],
        compiler_params=pltpu.CompilerParams(
            collective_id=0, has_side_effects=True, vmem_limit_bytes=vmem_bytes - out_bytes
        ),
    )(
        fwd_tokens, back_tokens, out_grad, norm_gain.reshape(1, width),
        gate_weight, up_weight, down_weight, gate_grad_sum,
    )


def body_for(mesh):
    def body(*args):
        tokens, width = args[0].shape
        depth, cols = args[4].shape
        rows = cols // 4
        fits = (
            mesh.shape["tp"] == 2 and mesh.shape["fs"] == 16
            and depth == 128 and width == 16 * depth and cols % 128 == 0 and tokens % 128 == 0
            and rows > 256 and rows % 16 == 0
        )
        if not fits:
            return shards(*args)
        return fused_shards((rows - 1) // 256 * 256, *args)

    return body


def solution(mesh):
    in_specs = (
        P("fs", None),
        P("fs", None),
        P("fs", None),
        P(),
        P("fs", "tp"),
        P("fs", "tp"),
        P("fs", "tp"),
        P("fs", "tp"),
    )
    out_specs = (P("fs", None), P("fs", None), P("fs", "tp"))
    return jax.shard_map(body_for(mesh), mesh=mesh, in_specs=in_specs, out_specs=out_specs, check_vma=False)
```

```python
import functools

import jax
import jax.numpy as jnp
from jax import lax
from jax.experimental import pallas as pl
from jax.experimental.pallas import tpu as pltpu
from jax.sharding import PartitionSpec as P

norm_eps = 0.25
vmem_bytes = 66_900_000


def normalize(tokens, norm_gain):
    values = tokens.astype(jnp.float32)
    factor = lax.rsqrt(jnp.mean(values * values, axis=-1, keepdims=True) + norm_eps)
    return (values, factor, (values * factor * norm_gain).astype(jnp.bfloat16))


def shards(
    fwd_tokens, back_tokens, out_grad, norm_gain, gate_weight, up_weight, down_weight, gate_grad_sum
):
    fwd_normed = normalize(fwd_tokens, norm_gain)[2]
    columns = fwd_normed
    gate_pre = jnp.dot(
        columns,
        lax.all_gather(gate_weight, "fs", axis=0, tiled=True),
        preferred_element_type=jnp.float32,
    )
    up_pre = jnp.dot(
        columns,
        lax.all_gather(up_weight, "fs", axis=0, tiled=True),
        preferred_element_type=jnp.float32,
    )
    hidden = (gate_pre * jax.nn.sigmoid(gate_pre) * up_pre).astype(jnp.bfloat16)
    partial_value = jnp.dot(
        hidden,
        lax.all_gather(down_weight, "fs", axis=0, tiled=True).T,
        preferred_element_type=jnp.float32,
    )
    summed = lax.psum(partial_value.astype(jnp.bfloat16), "tp").astype(jnp.float32)
    fwd_out = (0.5 * summed).astype(jnp.bfloat16)
    gate_whole = lax.all_gather(gate_weight, "fs", axis=0, tiled=True)
    up_whole = lax.all_gather(up_weight, "fs", axis=0, tiled=True)
    down_whole = lax.all_gather(down_weight, "fs", axis=0, tiled=True)
    values, factor, back_normed = normalize(back_tokens, norm_gain)
    gate_pre = jnp.dot(back_normed, gate_whole, preferred_element_type=jnp.float32)
    up_pre = jnp.dot(back_normed, up_whole, preferred_element_type=jnp.float32)
    sigmoid_gate = jax.nn.sigmoid(gate_pre)
    back_hidden = 0.5 * jnp.dot(out_grad, down_whole, preferred_element_type=jnp.float32)
    gate_diff = (
        back_hidden * up_pre * sigmoid_gate * (1.0 + gate_pre * (1.0 - sigmoid_gate))
    ).astype(jnp.bfloat16)
    up_diff = (back_hidden * gate_pre * sigmoid_gate).astype(jnp.bfloat16)
    columns = back_normed
    gate_grad_out = gate_grad_sum + lax.psum_scatter(
        jnp.dot(columns.T, gate_diff, preferred_element_type=jnp.float32),
        "fs",
        scatter_dimension=0,
        tiled=True,
    )
    partial_diff = jnp.dot(gate_diff, gate_whole.T, preferred_element_type=jnp.float32)
    partial_diff = partial_diff + jnp.dot(up_diff, up_whole.T, preferred_element_type=jnp.float32)
    normed_diff = lax.psum(partial_diff.astype(jnp.bfloat16), "tp").astype(jnp.float32)
    scaled = normed_diff * norm_gain
    cubed = factor * factor * factor
    back_grad = (
        factor * scaled - values * cubed * jnp.mean(scaled * values, axis=-1, keepdims=True)
    ).astype(jnp.bfloat16)
    back_grad, gate_grad_out = (back_grad, gate_grad_out)
    return (fwd_out, back_grad, gate_grad_out)


MESH = pl.DeviceIdType.MESH


def wide_dot(a, b):
    return lax.dot_general(a, b, (((1,), (1,)), ((), ())), preferred_element_type=jnp.float32)


def padded(size):
    return (size + 127) // 128 * 128


def layer_kernel(
    split, fwd_in, tokens_in, grad_in_ref, gain_ref, gate_in, up_in, down_in, sum_in,
    fwd_out, back_out, sum_out,
    raw, raw_tokens, sum_ref, turned, normed, toks, weights, staged, back_acc, down_acc, fwd_acc, hidden, diffs, diff_cols,
    part, crossed, joined, folded, gathered, grad_send, grad_side, grad_total, grad_pass, grad_recv, grad_turn, turn_recv, grad_cols,
    block_send, inner_send, line_recv, held_recv, side_recv, tok_send, tok_recv, relay_recv,
    gside_send, gside_recv, gsend, glev_recv, gpass_recv, gturn_recv,
    cross_send, cross_recv, join_send, fold_recv, join_recv, last_send, last_recv, raw_sem, token_sem, sum_sem,
):
    fs, core = lax.axis_index("fs"), lax.axis_index("tp")
    x, y, z = fs % 2, fs // 2 % 2, fs // 4
    odd = z % 2
    inner = jnp.logical_and(z > 0, z < 3)
    near, far, other = z + 1 - 2 * odd, (z + 2) % 4, 3 - z
    sibling = (fs, 1 - core)
    rows = turned.shape[1] // 4
    starts, sizes = (0, split), (split, rows - split)
    pads = tuple(padded(size) for size in sizes)
    depth = gate_in.shape[0]
    half = fwd_in.shape[0] // 2
    tokens_ref, fwd_ref, grad_ref = raw_tokens.at[0], raw_tokens.at[1], raw_tokens.at[2]
    slab = half * 4
    width = fwd_in.shape[1]
    band = 4 * depth

    def chip(to_x, to_y, to_z):
        return (to_z * 4 + to_y * 2 + to_x, core)

    beside, across = chip(1 - x, y, z), chip(x, 1 - y, z)
    y_flip = 1 - y

    barrier = pltpu.get_barrier_semaphore()
    for device in (
        sibling, beside, across, chip(x, y, near), chip(x, y, far), chip(x, y, other),
        chip(x, 1 - y, near), chip(x, 1 - y, far), chip(x, 1 - y, other),
    ):
        pl.semaphore_signal(barrier, inc=1, device_id=device, device_id_type=MESH)

    raw_copies = [pltpu.make_async_copy(ref, raw.at[w], raw_sem.at[w]) for w, ref in enumerate((gate_in, up_in, down_in))]
    token_copies = [
        pltpu.make_async_copy(ref, raw_tokens.at[a], token_sem.at[a]) for a, ref in enumerate((tokens_in, fwd_in, grad_in_ref))
    ]
    sum_copy = pltpu.make_async_copy(sum_in, sum_ref, sum_sem.at[0])
    for copy in (*raw_copies, token_copies[2], token_copies[0], token_copies[1], sum_copy):
        copy.start()

    def turn_in(w):
        raw_copies[w].wait()
        for n in range(turned.shape[1] // 128):
            at = pl.ds(n * 128, 128)
            turned[w, at, :] = raw[w, :, at].T

    def remote(src, dst, send, recv, device):
        return pltpu.make_async_remote_copy(
            src_ref=src, dst_ref=dst, send_sem=send, recv_sem=recv, device_id=device, device_id_type=MESH
        )

    def got(ref, sem):
        remote(ref, ref, sem, sem, sibling).wait_recv()

    def gone(ref, sem):
        remote(ref, ref, sem, sem, sibling).wait_send()

    def own_rows(h, to_y, to_odd):
        return pl.ds(pl.multiple_of((to_y * 2 + to_odd) * rows + starts[h], 16), sizes[h])

    def held_rows(w, h):
        return pl.ds(3 * starts[h] + w * pads[h], sizes[h])

    def both_rows(w, h, count=1):
        return pl.ds(3 * starts[h] + w * pads[h], count * pads[h])

    def own(w, h, to_y, to_odd):
        return turned.at[w, own_rows(h, to_y, to_odd), :]

    def lanes(src):
        return pl.ds(pl.multiple_of(src * depth, depth), depth)

    def level_lanes(s):
        return pl.ds(pl.multiple_of(s * band, band), band)

    def block(w, h, src):
        return weights.at[held_rows(w, h), lanes(src)]

    def send_block(w, h, src, source, device, recv, send):
        return remote(source, block(w, h, src), send.at[0], recv, device)

    def line_sem(w, h, role):
        return line_recv.at[w if h == 0 else 3, role]

    def held_sem(w, h):
        return held_recv.at[w if h == 0 else 3]

    def block_in(w, h, sem):
        if h == 0:
            got(weights.at[pl.ds(0, sizes[0]), pl.ds(0, depth)], sem)
        elif w == 0:
            got(weights.at[pl.ds(0, 3 * sizes[1]), pl.ds(0, depth)], sem)

    def to_near(w, h, src, source, line):
        send_block(w, h, src, source, chip(x, y, near), line_sem(w, h, 1 + line), block_send).start()

    def to_far(w, h, src, source, line):
        send_block(w, h, src, source, chip(x, y, far), line_sem(w, h, 3 + line), block_send).start()

    def to_other(w, h, src, source, line):
        @pl.when(inner)
        def _():
            send_block(w, h, src, source, chip(x, y, other), line_sem(w, h, 5 + line), inner_send).start()

    def pass_far(w, h, src, source, line):
        @pl.when(inner)
        def _():
            send_block(w, h, src, source, chip(x, y, far), line_sem(w, h, 5 + line), inner_send).start()

    def side(w, h, src, source, bundle):
        send_block(w, h, src, source, beside, side_recv.at[h, bundle], block_send).start()

    def send_stage(h, some=range(3)):
        for w in some:
            send_block(w, h, fs, own(w, h, 1 - y, odd), across, line_sem(w, h, 0), block_send).start()
            remote(
                own(w, h, 1 - y, 1 - odd), staged.at[held_rows(w, h), :], block_send.at[0], held_sem(w, h), across
            ).start()

    def send_own(h, some=range(3)):
        for w in some:
            to_near(w, h, fs, own(w, h, y, 1 - odd), 0)
            to_far(w, h, fs, own(w, h, y, odd), 0)
            side(w, h, fs, own(w, h, y, odd), 0)

    def send_others(h):
        for w in range(3):
            to_other(w, h, fs, own(w, h, y, 1 - odd), 0)
        for w in range(3):
            to_other(w, h, z * 4 + (1 - y) * 2 + x, staged.at[held_rows(w, h), :], 1)

    def keep_own(h):
        for w in range(3):
            weights[held_rows(w, h), lanes(fs)] = turned[w, own_rows(h, y, odd), :]

    def clear_pads():
        for h in range(2):
            if pads[h] > sizes[h]:
                for w in range(3):
                    gap = pl.ds(3 * starts[h] + w * pads[h] + sizes[h], pads[h] - sizes[h])
                    weights[gap, :] = jnp.zeros((pads[h] - sizes[h], width), jnp.bfloat16)

    def stage_in(w, h):
        src = z * 4 + (1 - y) * 2 + x
        held = staged.at[held_rows(w, h), :]
        block_in(w, h, held_sem(w, h))
        to_near(w, h, src, held, 1)
        block_in(w, h, line_sem(w, h, 0))
        to_far(w, h, src, block(w, h, src), 1)
        side(w, h, src, block(w, h, src), 0)

    def line_in(h, group, passed=None):
        s, line, role, bundle = group
        for w in range(3):
            src = s * 4 + line * 2 + x
            block_in(w, h, line_sem(w, h, role))
            if passed is not None:
                pass_far(w, h, src, block(w, h, src), passed)
            side(w, h, src, block(w, h, src), bundle)

    def sides_in(h, groups):
        got(weights.at[pl.ds(0, 3 * sizes[h]), pl.ds(0, len(groups) * depth)], side_recv.at[h, groups[0][3]])

    me = y * 2 + odd
    at_near, at_across, at_both = y * 2 + 1 - odd, (1 - y) * 2 + odd, (1 - y) * 2 + 1 - odd

    def token_rows(a, at):
        return grad_ref.at[at, :] if a == 2 else normed.at[a, at, :]

    def tok_block(a, h, q, n=None):
        rows_of = half if n is None else half // 2
        first = h * slab + q * half + (0 if n is None else n * rows_of)
        return toks.at[a, pl.ds(pl.multiple_of(first, rows_of), rows_of), :]

    def tok_copy(a, q, source, device, role, n=None):
        return remote(source, tok_block(a, core, q, n), tok_send.at[0], tok_recv.at[a, role], device)

    def relay(a, q, n=None):
        block_of = tok_block(a, core, q, n)
        return remote(block_of, block_of, tok_send.at[0], relay_recv.at[a], sibling)

    def tok_pieces(a):
        return (None,) if a != 1 else (0, 1)

    def send_tokens(a, role):
        for n in tok_pieces(a) if role == 0 else (None,):
            rows_of = half if n is None else half // 2
            mine = token_rows(a, pl.ds(pl.multiple_of(core * half + (n or 0) * rows_of, rows_of), rows_of))
            tok_copy(a, me, mine, (chip(x, y, near), across)[role], role + 3 * (n or 0), n).start()

    def normal(a):
        @pl.loop(0, tokens_ref.shape[0] // 16)
        def _(r):
            at = pl.ds(pl.multiple_of(r * 16, 16), 16)
            normed[a, at, :] = normalize((tokens_ref, fwd_ref)[a][at, :], gain_ref[...])[2]

    def keep_tokens(a):
        for h in range(2):
            toks[a, pl.ds(pl.multiple_of(h * slab + me * half, half), half), :] = token_rows(a, pl.ds(h * half, half))[...]

    def tok_in(a, q):
        role = [q is at for at in (at_near, at_across, at_both)].index(True)
        for n in tok_pieces(a) if role != 1 else (None,):
            got(tok_block(a, core, q, n), tok_recv.at[a, role + 3 * (n or 0)])
            if role == 0:
                tok_copy(a, q, tok_block(a, core, q, n), across, 2 + 3 * (n or 0), n).start()
            relay(a, q, n).start()

    def relayed(a):
        got(toks.at[a, pl.ds(0, 3 * half), :], relay_recv.at[a])

    def project(h, kind, groups, first=False):
        a, w, count, into = ((0, 0, 2, back_acc), (2, 2, 1, down_acc), (1, 0, 2, fwd_acc))[kind]
        wide = count * pads[h]
        at_rows = both_rows(w, h, count)
        for t in range(2):
            at_tokens = pl.ds(t * slab, slab)
            value = None if first else into[h, at_tokens, :wide]
            for s, line, _, _ in groups:
                at = pl.ds(pl.multiple_of((s * 4 + line * 2) * depth, 2 * depth), 2 * depth)
                term = wide_dot(toks[a, at_tokens, at], weights[at_rows, at])
                value = term if value is None else value + term
            into[h, at_tokens, :wide] = value

    piece = 64

    def back_parts(h):
        n = pads[h]

        @pl.loop(0, 2 * slab // piece)
        def _(r):
            at = pl.ds(pl.multiple_of(r * piece, piece), piece)
            gate, up = back_acc[h, at, :n], back_acc[h, at, n : 2 * n]
            s = jax.nn.sigmoid(gate)
            back = 0.5 * down_acc[h, at, :n]
            gate_diff = (back * up * s * (1.0 + gate * (1.0 - s))).astype(jnp.bfloat16)
            diff_cols[h, at, :n] = gate_diff
            diffs[h, at, :n] = gate_diff
            diffs[h, at, n : 2 * n] = (back * gate * s).astype(jnp.bfloat16)

    def fwd_parts(h):
        n = pads[h]

        @pl.loop(0, 2 * slab // piece)
        def _(r):
            at = pl.ds(pl.multiple_of(r * piece, piece), piece)
            gate, up = fwd_acc[h, at, :n], fwd_acc[h, at, n : 2 * n]
            hidden[h, at, :n] = (gate * jax.nn.sigmoid(gate) * up).astype(jnp.bfloat16)

    def grad_rows(h):
        return pl.ds(starts[h], sizes[h])

    def grad_across(h, n):
        pair = pl.ds((other, far, near, z)[n] * 2, 2)
        return remote(
            grad_send.at[1 - x, pair, grad_rows(h)], grad_side.at[pair, grad_rows(h)], gside_send.at[0], gside_recv.at[h, n], beside
        )

    def grad_make(h):
        diff_turned = diff_cols[h, :, : sizes[h]].T
        for s in range(4):
            at = level_lanes(s)
            product = jnp.dot(diff_turned, toks[0, :, at], preferred_element_type=jnp.float32)
            product = product.astype(jnp.bfloat16)
            for q in range(4):
                grad_send[q % 2, s * 2 + q // 2, grad_rows(h), :] = product[:, q * depth : (q + 1) * depth]

    def grad_out(h):
        for s in range(4):
            grad_across(h, s).start()

    def grad_to(h, n):
        s = (near, far, other)[n]
        source = grad_total.at[pl.ds(s * 2, 2), grad_rows(h)]
        return remote(source, grad_recv.at[n, :, grad_rows(h)], gsend.at[0], glev_recv.at[h, n], chip(x, y, s))

    def grad_past(h):
        source = grad_total.at[pl.ds(other * 2, 2), grad_rows(h)]
        return remote(source, grad_pass.at[:, grad_rows(h)], gsend.at[0], gpass_recv.at[h], chip(x, y, far))

    def grad_turned(h):
        return remote(
            grad_turn.at[:, grad_rows(h)], turn_recv.at[:, grad_rows(h)], gsend.at[0], gturn_recv.at[h], across
        )

    def grad_on(h, n):
        grad_across(h, n).wait_recv()
        for line in range(2):
            j = (other, far, near, z)[n] * 2 + line
            total = grad_send[x, j, grad_rows(h), :].astype(jnp.float32) + grad_side[j, grad_rows(h), :].astype(jnp.float32)
            grad_total[j, grad_rows(h), :] = total.astype(jnp.bfloat16)
        if n == 0:

            @pl.when(inner)
            def _():
                grad_to(h, 2).start()

            @pl.when(jnp.logical_not(inner))
            def _():
                grad_past(h).start()

        if n == 1:
            grad_to(h, 1).start()
        if n == 2:

            @pl.when(jnp.logical_not(inner))
            def _():
                grad_to(h, 0).start()

    def grad_mid(h):
        @pl.when(inner)
        def _():
            grad_past(h).wait_recv()
            for line in range(2):
                j = near * 2 + line
                total = grad_total[j, grad_rows(h), :].astype(jnp.float32) + grad_pass[line, grad_rows(h), :].astype(jnp.float32)
                grad_total[j, grad_rows(h), :] = total.astype(jnp.bfloat16)
            grad_to(h, 0).start()

    def grad_cols_at(h, to_y, to_odd):
        return pl.ds(pl.multiple_of((to_y * 2 + to_odd) * rows + starts[h], 16), sizes[h])

    def grad_cross(h):
        at = grad_rows(h)
        for n in range(2):
            grad_to(h, n).wait_recv()

        @pl.when(inner)
        def _():
            grad_to(h, 2).wait_recv()
            for line in range(2):
                total = grad_recv[0, line, at, :].astype(jnp.float32) + grad_recv[2, line, at, :].astype(jnp.float32)
                grad_recv[0, line, at, :] = total.astype(jnp.bfloat16)

        def sums(line):
            same = grad_total[z * 2 + line, at, :].astype(jnp.float32) + grad_recv[1, line, at, :].astype(jnp.float32)
            return same, grad_recv[0, line, at, :]

        same, unlike = sums(1 - y)
        grad_turn[0, at, :] = same.astype(jnp.bfloat16)
        grad_turn[1, at, :] = unlike
        grad_turned(h).start()
        same, unlike = sums(y)
        grad_cols[grad_cols_at(h, y, odd), :] = same
        grad_cols[grad_cols_at(h, y, 1 - odd), :] = unlike.astype(jnp.float32)

    def grad_in(h):
        grad_turned(h).wait_recv()
        for n, to_odd in enumerate((odd, 1 - odd)):
            grad_cols[grad_cols_at(h, 1 - y, to_odd), :] = turn_recv[n, grad_rows(h), :].astype(jnp.float32)

    span = width // 2

    def columns(c):
        return pl.ds(c * span, span)

    def cross(k, c):
        at = columns(c)
        return remote(
            part.at[k, 1 - core, :, at], crossed.at[k, :, at], cross_send.at[0], cross_recv.at[k, c], sibling
        )

    strip = 512

    def product_of(k, h, rows_at, at):
        n = pads[h]
        if k == 0:
            return jnp.dot(hidden[h, rows_at, :n], weights[both_rows(2, h), at], preferred_element_type=jnp.float32)
        return jnp.dot(diffs[h, rows_at, : 2 * n], weights[both_rows(0, h, 2), at], preferred_element_type=jnp.float32)

    def partial(k, t, c):
        rows_at = pl.ds(pl.multiple_of(t * slab, slab), slab)
        at = columns(c)
        part[k, t, :, at] = (product_of(k, 0, rows_at, at) + product_of(k, 1, rows_at, at)).astype(jnp.bfloat16)

    routes = ((across, at_across, at_near, chip(x, y, near)), (chip(x, y, near), at_near, at_across, across))
    routed = ((0, 0), (1, 0))
    def join_copy(k, c, n):
        to, theirs, mine, on = routes[routed[k][c]]
        at = columns(c)
        if n == 2:
            source, device = folded.at[k, :, at], on
        else:
            source, device = joined.at[k, (at_both, theirs)[n], :, at], to
        recv = fold_recv.at[k, c] if n == 0 else join_recv.at[k]
        return remote(source, gathered.at[k, n, :, at], join_send.at[0], recv, device)

    def join_start(k, c):
        if c == 0:
            return
        for c in range(2):
            cross(k, c).wait_recv()
        for n in range(4):
            for c in range(2):
                at = columns(c)
                q = (at_both, *routes[routed[k][c]][1:3], me)[n]
                rows_at = pl.ds(pl.multiple_of(q * half, half), half)
                total = part[k, core, rows_at, at].astype(jnp.float32) + crossed[k, rows_at, at].astype(jnp.float32)
                joined[k, q, :, at] = total.astype(jnp.bfloat16)
                if n < 2:
                    join_copy(k, c, n).start()

    def join_fold(k, c):
        at = columns(c)
        join_copy(k, c, 0).wait_recv()
        total = gathered[k, 0, :, at].astype(jnp.float32) + joined[k, routes[routed[k][c]][2], :, at].astype(jnp.float32)
        folded[k, :, at] = total.astype(jnp.bfloat16)
        join_copy(k, c, 2).start()

    def stages_in(h):
        for w in range(3):
            stage_in(w, h)

    first_far = (jnp.where(inner, other, far), jnp.where(inner, y, y_flip), jnp.where(inner, 5, 4), 1)
    next_far = (other, jnp.where(inner, y_flip, y), jnp.where(inner, 6, 5), 2)
    last_far = (jnp.where(inner, far, other), y_flip, jnp.where(inner, 4, 6), 2)
    near_own, near_across, far_own = (near, y, 1, 1), (near, y_flip, 2, 2), (far, y, 3, 1)
    lead = (jnp.where(inner, near, far), jnp.where(inner, y, y_flip), jnp.where(inner, 1, 4), 1)
    follow = (jnp.where(inner, other, near), y, jnp.where(inner, 5, 1), 1)
    home = ((z, y, 0, 0), (z, y_flip, 0, 0))
    soon = (near_own, far_own, first_far)
    late = (near_across, next_far, last_far)

    def down_parts(k):
        for c in range(2):
            partial(k, 1 - core, c)
            cross(k, c).start()
        for c in range(2):
            partial(k, core, c)

    for w in range(3):
        turn_in(w)
        if w == 0:
            pl.semaphore_wait(barrier, 9)
        send_stage(0, (w,))
        send_own(0, (w,))
    token_copies[2].wait()
    send_tokens(2, 1)
    send_tokens(2, 0)
    token_copies[0].wait()
    normal(0)
    send_tokens(0, 1)
    send_tokens(0, 0)
    send_own(1)
    token_copies[1].wait()
    normal(1)
    clear_pads()
    for h in range(2):
        keep_own(h)
    for a in range(3):
        keep_tokens(a)
    stages_in(0)
    line_in(0, far_own)
    line_in(0, lead, 0)
    send_others(0)
    send_stage(1)
    tok_in(2, at_across)

    @pl.when(inner)
    def _():
        tok_in(2, at_near)

    line_in(0, follow)

    @pl.when(jnp.logical_not(inner))
    def _():
        tok_in(2, at_near)

    tok_in(0, at_across)
    line_in(1, far_own)

    @pl.when(inner)
    def _():
        tok_in(0, at_near)

    stages_in(1)
    send_tokens(1, 0)
    send_others(1)
    line_in(0, next_far)

    @pl.when(jnp.logical_not(inner))
    def _():
        tok_in(0, at_near)

    send_tokens(1, 1)
    line_in(1, near_own, 0)
    tok_in(2, at_both)
    line_in(0, near_across, 1)
    relayed(2)
    line_in(1, first_far)
    sides_in(0, home)
    project(0, 1, home, True)
    tok_in(0, at_both)
    line_in(1, next_far)
    relayed(0)
    project(0, 0, home, True)
    tok_in(1, at_across)
    sides_in(0, soon)
    project(0, 1, soon)
    line_in(0, last_far)
    project(0, 0, soon)

    @pl.when(inner)
    def _():
        tok_in(1, at_near)

    sides_in(1, home)
    project(1, 0, home, True)
    project(1, 1, home, True)
    line_in(1, near_across, 1)
    line_in(1, last_far)
    sides_in(1, soon)
    project(1, 0, soon)
    project(1, 1, soon)
    sides_in(0, late)
    project(0, 1, late)
    project(0, 0, late)
    back_parts(0)
    grad_make(0)
    grad_out(0)

    @pl.when(jnp.logical_not(inner))
    def _():
        tok_in(1, at_near)

    sides_in(1, late)
    project(1, 0, late)
    project(1, 1, late)
    back_parts(1)
    down_parts(1)
    for c in range(2):
        join_start(1, c)
    tok_in(1, at_both)
    grad_on(0, 0)
    relayed(1)
    project(0, 2, home + soon + late, True)
    fwd_parts(0)
    grad_on(0, 1)
    project(1, 2, home + soon + late, True)
    fwd_parts(1)
    down_parts(0)
    grad_on(0, 2)
    for c in range(2):
        join_start(0, c)
    grad_make(1)
    grad_out(1)
    for c in range(2):
        join_fold(1, c)
    grad_on(0, 3)
    grad_mid(0)
    for n in range(4):
        grad_on(1, n)
    for c in range(2):
        join_fold(0, c)
    grad_mid(1)
    grad_cross(0)
    grad_cross(1)

    mine = pl.ds(pl.multiple_of(core * half, half), half)

    def last(k):
        out = (fwd_out, back_out)[k].at[mine, :]
        return remote(out, out, last_send.at[0], last_recv.at[0], sibling)

    def joined_in(k):
        got(gathered.at[k, pl.ds(1, 2)], join_recv.at[k])

    def total_of(k, at):
        value = joined[k, me, at, :].astype(jnp.float32) + gathered[k, 1, at, :].astype(jnp.float32)
        return value + gathered[k, 2, at, :].astype(jnp.float32)

    tiles = grad_cols.shape[0] // 128
    early = rows * 2 // 128

    def grad_tiles(first, count):
        for n in range(count):
            at = pl.ds(pl.multiple_of((first + n) * 128, 128), 128)
            sum_out[:, at] = sum_ref[:, at] + grad_cols[at, :].T

    small = 16

    def out_rows(r):
        return pl.ds(pl.multiple_of(core * half + r * small, small), small)

    sum_copy.wait()
    grad_tiles(y * (tiles - early), early)
    joined_in(0)
    for r in range(half // small):
        fwd_out[out_rows(r), :] = (0.5 * total_of(0, pl.ds(r * small, small))).astype(jnp.bfloat16)
    last(0).start()
    joined_in(1)
    for r in range(half // small):
        values = tokens_ref[out_rows(r), :].astype(jnp.float32)
        factor = lax.rsqrt(jnp.mean(values * values, axis=-1, keepdims=True) + norm_eps)
        scaled = total_of(1, pl.ds(r * small, small)) * gain_ref[...]
        cubed = factor * factor * factor
        back_out[out_rows(r), :] = (
            factor * scaled - values * cubed * jnp.mean(scaled * values, axis=-1, keepdims=True)
        ).astype(jnp.bfloat16)
    last(1).start()

    for h in range(2):
        grad_in(h)
    grad_tiles((1 - y) * early, tiles - early)

    gone(weights.at[pl.ds(0, 3 * rows), pl.ds(0, 14 * depth)], block_send.at[0])

    @pl.when(inner)
    def _():
        gone(weights.at[pl.ds(0, 3 * rows), pl.ds(0, 4 * depth)], inner_send.at[0])

    gone(toks.at[:, pl.ds(0, 6 * half), :], tok_send.at[0])
    gone(grad_side, gside_send.at[0])
    gone(grad_total, gsend.at[0])
    gone(part.at[0], cross_send.at[0])
    gone(joined.at[:, pl.ds(0, 3)], join_send.at[0])
    gone(fwd_out, last_send.at[0])
    got(fwd_out, last_recv.at[0])


def fused_shards(
    split, fwd_tokens, back_tokens, out_grad, norm_gain, gate_weight, up_weight, down_weight, gate_grad_sum
):
    tokens, width = fwd_tokens.shape
    depth, cols = gate_weight.shape
    rows = cols // 4
    out_bytes = 2 * tokens * width * 2 + depth * cols * 4
    wide = max(padded(split), padded(rows - split))
    held = 3 * (padded(split) + padded(rows - split))
    half = tokens // 2
    slab = half * 4
    narrow, full = jnp.bfloat16, jnp.float32
    dma = pltpu.SemaphoreType.DMA
    vmem = pl.BlockSpec(memory_space=pltpu.VMEM)
    hbm = pl.BlockSpec(memory_space=pl.ANY)
    return pl.pallas_call(
        functools.partial(layer_kernel, split),
        out_shape=(
            pltpu.VMEM((tokens, width), narrow),
            pltpu.VMEM((tokens, width), narrow),
            pltpu.VMEM((depth, cols), full),
        ),
        in_specs=[hbm] * 3 + [vmem] + [hbm] * 4,
        out_specs=(vmem,) * 3,
        scratch_shapes=[
            pltpu.VMEM((3, depth, cols), narrow),
            pltpu.VMEM((3, tokens, width), narrow),
            pltpu.VMEM((depth, cols), full),
            pltpu.VMEM((3, cols, depth), narrow),
            pltpu.VMEM((2, tokens, width), narrow),
            pltpu.VMEM((3, 2 * slab, width), narrow),
            pltpu.VMEM((held, width), narrow),
            pltpu.VMEM((held, depth), narrow),
            pltpu.VMEM((2, 2 * slab, 2 * wide), full),
            pltpu.VMEM((2, 2 * slab, wide), full),
            pltpu.VMEM((2, 2 * slab, 2 * wide), full),
            pltpu.VMEM((2, 2 * slab, wide), narrow),
            pltpu.VMEM((2, 2 * slab, 2 * wide), narrow),
            pltpu.VMEM((2, 2 * slab, wide), narrow),
            pltpu.VMEM((2, 2, slab, width), narrow),
            pltpu.VMEM((2, slab, width), narrow),
            pltpu.VMEM((2, 4, half, width), narrow),
            pltpu.VMEM((2, half, width), narrow),
            pltpu.VMEM((2, 3, half, width), narrow),
            pltpu.VMEM((2, 8, rows, depth), narrow),
            pltpu.VMEM((8, rows, depth), narrow),
            pltpu.VMEM((8, rows, depth), narrow),
            pltpu.VMEM((2, rows, depth), narrow),
            pltpu.VMEM((3, 2, rows, depth), narrow),
            pltpu.VMEM((2, rows, depth), narrow),
            pltpu.VMEM((2, rows, depth), narrow),
            pltpu.VMEM((cols, depth), full),
            dma((1,)),
            dma((1,)),
            dma((4, 7)),
            dma((4,)),
            dma((2, 3)),
            dma((1,)),
            dma((3, 6)),
            dma((3,)),
            dma((1,)),
            dma((2, 4)),
            dma((1,)),
            dma((2, 3)),
            dma((2,)),
            dma((2,)),
            dma((1,)),
            dma((2, 2)),
            dma((1,)),
            dma((2, 2)),
            dma((2,)),
            dma((1,)),
            dma((1,)),
            dma((3,)),
            dma((3,)),
            dma((1,)),
        ],
        compiler_params=pltpu.CompilerParams(
            collective_id=0, has_side_effects=True, vmem_limit_bytes=vmem_bytes - out_bytes
        ),
    )(
        fwd_tokens, back_tokens, out_grad, norm_gain.reshape(1, width),
        gate_weight, up_weight, down_weight, gate_grad_sum,
    )


def body_for(mesh):
    def body(*args):
        tokens, width = args[0].shape
        depth, cols = args[4].shape
        rows = cols // 4
        fits = (
            mesh.shape["tp"] == 2 and mesh.shape["fs"] == 16
            and depth == 128 and width == 16 * depth and cols % 128 == 0 and tokens % 128 == 0
            and rows > 256 and rows % 16 == 0
        )
        if not fits:
            return shards(*args)
        return fused_shards((rows - 1) // 256 * 256, *args)

    return body


def solution(mesh):
    in_specs = (
        P("fs", None),
        P("fs", None),
        P("fs", None),
        P(),
        P("fs", "tp"),
        P("fs", "tp"),
        P("fs", "tp"),
        P("fs", "tp"),
    )
    out_specs = (P("fs", None), P("fs", None), P("fs", "tp"))
    return jax.shard_map(body_for(mesh), mesh=mesh, in_specs=in_specs, out_specs=out_specs, check_vma=False)
```
